512 devices in a mesh: grp: 2 (over y), dp: 8 (over x), kv: 16 (over z), tp: 2 (over core).
Axes of the slice: x: 8, y: 2, z: 16, core: 2. Of those that a mesh axis runs over, the one named last changes fastest.
The devices are a block of a 8x8x16 slice.
Arguments:
- tokens: bfloat16 [384, 4, 4096], P(('grp', 'dp'), None, ('kv', 'tp')), parts along dimension 0, may hold values from -6 to 6
- norm_gain: float32 [4096], replicated, may hold values from 0.1 to 1.9
- w_query: bfloat16 [16, 128, 4096], P('kv', 'tp'), may hold values from -0.09375 to 0.09375
- w_key: bfloat16 [16, 128, 4096], P('kv', 'tp'), may hold values from -0.09375 to 0.09375
- w_value: bfloat16 [16, 128, 4096], P('kv', 'tp'), may hold values from -0.09375 to 0.09375
- w_gate: bfloat16 [16, 128, 4096], P('kv', 'tp'), may hold values from -0.09375 to 0.09375
- w_decay: bfloat16 [4096, 16], replicated, may hold values from -0.09375 to 0.09375
- w_beta: bfloat16 [4096, 16], replicated, may hold values from -0.09375 to 0.09375
- decay_rate: float32 [16], P('kv'), may hold values from 0.02 to 1
- head_gain: float32 [128], P('tp'), may hold values from 0.1 to 1.9
- w_out: bfloat16 [16, 128, 4096], P('kv', 'tp'), may hold values from -0.1875 to 0.1875
- state: float32 [384, 16, 128, 128], P(('grp', 'dp'), 'kv', 'tp'), parts along dimension 0, may hold values from -6 to 6
- prev_keys: bfloat16 [384, 4, 16, 128], P(('grp', 'dp'), None, 'kv'), parts along dimension 0, may hold values from -6 to 6
- prev_values: bfloat16 [384, 4, 16, 128], P(('grp', 'dp'), None, 'kv', 'tp'), parts along dimension 0, may hold values from -6 to 6
- prev_decay: float32 [384, 4, 16], P(('grp', 'dp'), None, 'kv'), parts along dimension 0, may hold values from 0.01 to 1
- prev_beta: float32 [384, 4, 16], P(('grp', 'dp'), None, 'kv'), parts along dimension 0, may hold values from 0.05 to 1
- accepted: int32 [384], P(('grp', 'dp')), parts along dimension 0, may hold values from 0 to 4
Outputs:
- mixed: bfloat16 [384, 4, 4096], P(('grp', 'dp'), None, ('kv', 'tp')), parts along dimension 0
- committed: float32 [384, 16, 128, 128], P(('grp', 'dp'), 'kv', 'tp'), parts along dimension 0
The draws below stay inside these ranges and needn't reach their ends.
There are 2 independent parts, one for each index of `grp`. The reference program is written for one: setup_inputs(seed, part) draws one part's arguments, and reference() takes and returns one part's arrays. A program takes and returns all parts, laid end to end along the dimension named above; an argument that names none is the same for every part. Nothing has to cross between parts.
All inputs are finite; a program needn't handle non-finite values.
Results may differ from the reference program's by a relative error of at most 0.015.
Values may be sent and summed in bfloat16 or wider, within the bound.
No kernel may reach another device: no remote copies, remote signals or barrier semaphores. Data moves between devices by JAX's collectives and lax.ppermute only.
A program may use at most 64 MiB of HBM per device.

```python
import math
import jax
import jax.numpy as jnp
from jax import lax

D = 4096
H = 16
DK = 128
DV = 128
P_SIZE = 4
SEQS = 192


def touch_ends(drawn, own_key, least, largest):
    extent = drawn.shape
    spot = [jax.random.randint(jax.random.fold_in(own_key, axis), (), 0, extent[axis]) for axis in range(len(extent))]
    drawn = drawn.at[tuple(spot)].set(least)
    longest = extent.index(max(extent))
    spot[longest] = (spot[longest] + 1) % extent[longest]
    return drawn.at[tuple(spot)].set(largest)


def with_spikes(drawn, own_key, source, target, parts, factor):
    owner, partner = [(jnp.arange(drawn.shape[axis_at]) // (drawn.shape[axis_at] // parts)).reshape([-1 if axis == axis_at else 1 for axis in range(drawn.ndim)]) for axis_at in (source, target)]
    chosen = jax.random.permutation(own_key, parts)[partner]
    strong = (owner == chosen) | (owner == (partner + parts // 2) % parts)
    return jnp.where(strong, factor * drawn, drawn)


def shard_levels(own_key, dims, shards, least, top_value):
    loudness, own = 1.0, jax.random.fold_in(own_key, 6)
    for axis_at, blocks in shards:
        steps = jnp.exp(jax.random.uniform(jax.random.fold_in(own, axis_at), (blocks,), jnp.float32, least / len(shards), top_value / len(shards)))
        loudness = loudness * jnp.repeat(steps, dims[axis_at] // blocks).reshape([-1 if axis == axis_at else 1 for axis in range(len(dims))])
    return loudness


def gaussian(rng, shape, deviation, bound, split=(), held_as=jnp.bfloat16):
    loudness = shard_levels(rng, shape, split, -0.22, 0.18) if split else 1.0
    drawn = jax.random.normal(rng, shape, jnp.float32) * deviation * loudness
    return jnp.minimum(jnp.maximum(drawn, -bound), bound).astype(held_as)


def heavy_noise(key, dims, width, bound, split, heavy, kind=jnp.bfloat16):
    array = width * jax.random.normal(key, dims, jnp.float32)
    if split:
        array = array * shard_levels(key, dims, split, -0.22, 0.18)
    return jnp.clip(with_spikes(array, jax.random.fold_in(key, 3), *heavy), -bound, bound).astype(kind)


def setup_inputs(seed: int = 0, part: int = 0) -> dict:
    streams_of = jax.random.split(jax.random.key(seed), 18)
    part_keys = jax.random.split(jax.random.fold_in(streams_of[17], part), 18)
    return {
        "tokens": gaussian(part_keys[0], (SEQS, P_SIZE, D), 1.0, 6.0, ((0, 8), (2, 32))),
        "norm_gain": jnp.clip(1.0 + 0.18 * jax.random.normal(streams_of[1], (D,), jnp.float32), 0.1, 1.9),
        "w_query": gaussian(streams_of[2], (H, DK, D), D ** -0.5, 0.09375, ((0, 16), (1, 2))),
        "w_key": gaussian(streams_of[3], (H, DK, D), D ** -0.5, 0.09375, ((0, 16), (1, 2))),
        "w_value": gaussian(streams_of[4], (H, DV, D), D ** -0.5, 0.09375, ((0, 16), (1, 2))),
        "w_gate": gaussian(streams_of[5], (H, DV, D), D ** -0.5, 0.09375, ((0, 16), (1, 2))),
        "w_decay": gaussian(streams_of[6], (D, H), D ** -0.5, 0.09375),
        "w_beta": gaussian(streams_of[7], (D, H), D ** -0.5, 0.09375),
        "decay_rate": jnp.clip(jnp.exp(math.log(1.0) - 3.912023 * jax.random.uniform(streams_of[8], (H,), jnp.float32) ** shard_levels(streams_of[8], (H,), ((0, 16),), -0.2, 0.2)), 0.02, 1.0),
        "head_gain": jnp.clip(1.0 + 0.18 * jax.random.normal(streams_of[9], (DV,), jnp.float32), 0.1, 1.9),
        "w_out": heavy_noise(streams_of[10], (H, DV, D), (H * DV) ** -0.5, 0.1875, ((0, 16), (1, 2)), (0, 2, 16, 2.0)),
        "state": gaussian(part_keys[11], (SEQS, H, DV, DK), 1.0, 6.0, ((0, 8), (1, 16), (2, 2)), jnp.float32),
        "prev_keys": gaussian(part_keys[12], (SEQS, P_SIZE, H, DK), 1.0, 6.0, ((0, 8), (2, 16))),
        "prev_values": gaussian(part_keys[13], (SEQS, P_SIZE, H, DV), 1.0, 6.0, ((0, 8), (2, 16), (3, 2))),
        "prev_decay": jnp.clip(jnp.exp(math.log(1.0) - 4.6051702 * jax.random.uniform(part_keys[14], (SEQS, P_SIZE, H), jnp.float32) ** shard_levels(part_keys[14], (SEQS, P_SIZE, H), ((0, 8), (2, 16)), -0.2, 0.2)), 0.01, 1.0),
        "prev_beta": jnp.clip(0.05 + 0.95 * jax.random.uniform(part_keys[15], (SEQS, P_SIZE, H), jnp.float32) ** shard_levels(part_keys[15], (SEQS, P_SIZE, H), ((0, 8), (2, 16)), -0.2, 0.2), 0.05, 1.0),
        "accepted": touch_ends(jax.random.randint(part_keys[16], (SEQS,), 0, P_SIZE + 1), jax.random.fold_in(part_keys[16], 1), 0, P_SIZE).astype(jnp.int32),
    }


EPS = 1e-06
PRECISE = lax.Precision.HIGHEST

def unit_rows(values):
    return values * lax.rsqrt(lax.optimization_barrier(jnp.sum(values * values, axis=-1, keepdims=True)) + EPS)

def delta_update(carried, keys_now, values_now, retain, strength):
    carried = carried * retain[..., None, None]
    predicted = jnp.einsum('shed,shd->she', carried, keys_now, precision=PRECISE)
    update = strength[..., None] * (values_now - predicted)
    return carried + update[..., :, None] * keys_now[..., None, :]

def reference(tokens, norm_gain, w_query, w_key, w_value, w_gate, w_decay, w_beta, decay_rate, head_gain, w_out, state, prev_keys, prev_values, prev_decay, prev_beta, accepted):
    floats = tokens.astype(jnp.float32)
    normed = (floats * lax.rsqrt(lax.optimization_barrier(jnp.mean(floats * floats, axis=-1, keepdims=True)) + EPS) * norm_gain).astype(jnp.bfloat16)
    flat_rows = normed.reshape(SEQS * P_SIZE, D)

    def project(weight):
        product = lax.dot_general(flat_rows, weight.reshape(-1, D), (((1,), (1,)), ((), ())), preferred_element_type=jnp.float32)
        return product.astype(jnp.bfloat16).reshape(SEQS, P_SIZE, H, -1)
    query = project(w_query)
    key_raw = project(w_key)
    value_raw = project(w_value)
    gate_raw = project(w_gate)
    decay_pre = jnp.dot(flat_rows, w_decay, preferred_element_type=jnp.float32).reshape(SEQS, P_SIZE, H)
    beta_pre = jnp.dot(flat_rows, w_beta, preferred_element_type=jnp.float32).reshape(SEQS, P_SIZE, H)
    forget = decay_rate * jax.nn.softplus(decay_pre)
    strength = jax.nn.sigmoid(beta_pre)
    queries = unit_rows(jax.nn.silu(query.astype(jnp.float32))) * DK ** (-0.5)
    key_unit = unit_rows(jax.nn.silu(key_raw.astype(jnp.float32)))
    value_act = jax.nn.silu(value_raw.astype(jnp.float32))
    old_keys = unit_rows(prev_keys.astype(jnp.float32))
    old_values = prev_values.astype(jnp.float32)
    carried = state
    for position in range(P_SIZE):
        accept_mask = (position < accepted).astype(jnp.float32)[:, None]
        carried = delta_update(carried, old_keys[:, position], old_values[:, position], jnp.exp(-prev_decay[:, position] * accept_mask), prev_beta[:, position] * accept_mask)
    committed = carried
    outputs = []
    for position in range(P_SIZE):
        carried = delta_update(carried, key_unit[:, position], value_act[:, position], jnp.exp(-forget[:, position]), strength[:, position])
        outputs.append(jnp.einsum('shed,shd->she', carried, queries[:, position], precision=PRECISE))
    heads_out = jnp.stack(outputs, axis=1)
    scaled = (heads_out * lax.rsqrt(lax.optimization_barrier(jnp.mean(heads_out * heads_out, axis=-1, keepdims=True)) + EPS) * head_gain * jax.nn.silu(gate_raw.astype(jnp.float32))).astype(jnp.bfloat16)
    mixed_out = jnp.dot(scaled.reshape(SEQS * P_SIZE, H * DV), w_out.reshape(H * DV, D), preferred_element_type=jnp.float32).astype(jnp.bfloat16)
    return (mixed_out.reshape(SEQS, P_SIZE, D), committed)
```

```python
import jax
import jax.numpy as jnp
from jax import lax
from jax.experimental import pallas as pl
from jax.experimental.pallas import tpu as pltpu
from jax.sharding import PartitionSpec as P

EPS = 1e-06
F32 = jnp.float32
BF16 = jnp.bfloat16
SWAP = [(0, 1), (1, 0)]


def mm(a, b, dims=((1,), (0,))):
    return lax.dot_general(
        a.astype(BF16), b.astype(BF16), (dims, ((), ())), preferred_element_type=F32
    )


NT = ((1,), (1,))


def high(a, b):
    return lax.dot_general(
        a, b, (((1,), (0,)), ((), ())), precision=lax.Precision.HIGHEST, preferred_element_type=F32
    )


def silu(x):
    return x / (1.0 + jnp.exp(-x))


def turned(x):
    n = x.shape[1]
    eye = lax.broadcasted_iota(jnp.int32, (n, n), 0) == lax.broadcasted_iota(jnp.int32, (n, n), 1)
    return mm(jnp.where(eye, 1.0, 0.0), x, NT)


def decays(d_row, steps):
    n = d_row.shape[1]
    shift = steps.bit_length() - 1
    i = lax.broadcasted_iota(jnp.int32, (n, n), 0)
    r = lax.broadcasted_iota(jnp.int32, (n, n), 1)
    same = (i >> shift) == (r >> shift)
    upto = same & (i <= r)
    before = same & (i < r)
    d_col = jnp.sum(jnp.where(i == r, d_row, 0.0), axis=1, keepdims=True)
    g_row = jnp.sum(jnp.where(upto, d_col, 0.0), axis=0, keepdims=True)
    g_col = jnp.sum(jnp.where(i == r, g_row, 0.0), axis=1, keepdims=True)
    between = jnp.where(upto, jnp.exp(jnp.where(upto, g_row - g_col, 0.0)), 0.0)
    last = jnp.sum(jnp.where(same & ((i & (steps - 1)) == steps - 1), g_col, 0.0), axis=0, keepdims=True)
    return g_row, g_col, last, between, before


def solved(b, n):
    first = b - high(b, n)
    return first + high(first, high(n, n))


def own_products(states, keys_t, seqs, steps):
    product = mm(states, keys_t)
    rows, n = product.shape[0] // seqs, product.shape[1]
    shift = steps.bit_length() - 1
    seq_of = lax.broadcasted_iota(jnp.int32, (rows, n), 1) >> shift
    total = jnp.zeros((rows, n), F32)
    for s in range(seqs):
        total = total + jnp.where(seq_of == s, product[s * rows : (s + 1) * rows], 0.0)
    return total


def commit_kernel(state_ref, keys_ref, values_ref, rows_ref, out_ref, keep_ref, send_ref):
    seqs, rows, width = state_ref.shape
    n = keys_ref.shape[0]
    steps = n // seqs
    shift = steps.bit_length() - 1
    keys = keys_ref[...].astype(F32)
    keys = keys * lax.rsqrt(jnp.sum(keys * keys, axis=-1, keepdims=True) + EPS)
    keys_t = turned_f32(keys)
    d_row, b_row = -rows_ref[0:1, :], rows_ref[1:2, :]
    g_row, g_col, last, between, before = decays(d_row, steps)
    gram = mm(keys, keys, NT)
    nil = jnp.where(before, between * gram * b_row, 0.0)
    state = state_ref[...]
    known = own_products(state.reshape(seqs * rows, width), keys_t, seqs, steps)
    values_t = turned(values_ref[...])
    u = solved(b_row * (values_t - jnp.exp(g_row) * known), nil) * jnp.exp(last - g_row)
    seq_of = lax.broadcasted_iota(jnp.int32, (rows, n), 1) >> shift
    spread = jnp.concatenate([jnp.where(seq_of == s, u, 0.0).astype(BF16) for s in range(seqs)], axis=0)
    update = mm(spread, keys)
    kept = jnp.broadcast_to(jnp.exp(g_col), (n, width))
    for s in range(seqs):
        at = s * steps + steps - 1
        out_ref[s] = state[s] * kept[at : at + 1, :] + update[s * rows : (s + 1) * rows]
    half = seqs // 2
    tp = lax.axis_index("tp")
    keep_ref[...] = out_ref[pl.ds(tp * half, half)].astype(BF16)
    send_ref[...] = out_ref[pl.ds((1 - tp) * half, half)].astype(BF16)


def turned_f32(x):
    return turned(x.astype(BF16))


def layer_kernel(
    x_ref, gain_ref, wq_ref, wk_ref, wv_ref, wg_ref, wq2_ref, wk2_ref, wv2_ref, wg2_ref,
    decay_ref, beta_ref, rate_ref, hg_ref, hg2_ref, keep_ref, got_ref, wo_ref, wo2_ref, out_ref,
):
    blocks, _, n, lanes = x_ref.shape
    seqs, rows, width = keep_ref.shape
    steps = n // seqs
    heads = decay_ref.shape[0]
    tp = lax.axis_index("tp")
    head = lax.axis_index("kv")
    features = blocks * 2 * lanes
    squares = jnp.zeros((n, lanes), F32)
    for b in range(blocks):
        for c in range(2):
            part = x_ref[b, c].astype(F32)
            squares = squares + part * part
    scale = lax.rsqrt(jnp.sum(squares, axis=-1, keepdims=True) / features + EPS)
    mine = jnp.zeros((4 * rows, n), F32)
    others = jnp.zeros((4 * rows, n), F32)
    gates = jnp.zeros((2 * heads, n), F32)
    for b in range(blocks):
        at = slice(b * 2 * lanes, (b + 1) * 2 * lanes)
        pair = jnp.concatenate([x_ref[b, tp], x_ref[b, 1 - tp]], axis=1).astype(F32)
        gain = jnp.concatenate([gain_ref[2 * b : 2 * b + 1, :], gain_ref[2 * b + 1 : 2 * b + 2, :]], axis=1)
        normed = (pair * scale * gain).astype(BF16)
        w = jnp.concatenate([r[:, at] for r in (wq_ref, wk_ref, wv_ref, wg_ref)], axis=0)
        mine = mine + mm(w, normed, NT)
        w = jnp.concatenate([r[:, at] for r in (wq2_ref, wk2_ref, wv2_ref, wg2_ref)], axis=0)
        others = others + mm(w, normed, NT)
        w = jnp.concatenate([decay_ref[:, at], beta_ref[:, at]], axis=0)
        gates = gates + mm(w, normed, NT)
    mine = mine.astype(BF16).astype(F32)
    others = others.astype(BF16).astype(F32)

    def in_order(k):
        a, b = mine[k * rows : (k + 1) * rows], others[k * rows : (k + 1) * rows]
        return jnp.where(tp == 0, jnp.concatenate([a, b], axis=0), jnp.concatenate([b, a], axis=0))

    def own_first(k):
        return jnp.concatenate([mine[k * rows : (k + 1) * rows], others[k * rows : (k + 1) * rows]], axis=0)

    def unit(u):
        return u * lax.rsqrt(jnp.sum(u * u, axis=0, keepdims=True) + EPS)

    query = unit(silu(in_order(0))) * width ** (-0.5)
    key = unit(silu(in_order(1)))
    value = silu(own_first(2))
    gate = silu(own_first(3))
    at_head = lax.broadcasted_iota(jnp.int32, (heads, n), 0) == head
    decay_pre = jnp.sum(jnp.where(at_head, gates[:heads], 0.0), axis=0, keepdims=True)
    beta_pre = jnp.sum(jnp.where(at_head, gates[heads:], 0.0), axis=0, keepdims=True)
    softplus = jnp.maximum(decay_pre, 0.0) + jnp.log1p(jnp.exp(-jnp.abs(decay_pre)))
    d_row = -rate_ref[0] * softplus
    b_row = 1.0 / (1.0 + jnp.exp(-beta_pre))
    g_row, _, _, between, before = decays(d_row, steps)

    kept = keep_ref[...].reshape(seqs * rows, width)
    got = got_ref[...].reshape(seqs * rows, width)

    def from_states(u):
        return jnp.concatenate([own_products(c, u, seqs, steps) for c in (kept, got)], axis=0)

    key_rows = turned_f32(key)
    nil = jnp.where(before, between * mm(key_rows, key) * b_row, 0.0)
    u = solved(b_row * (value - jnp.exp(g_row) * from_states(key)), nil)
    o = jnp.exp(g_row) * from_states(query) + high(u, between * mm(key_rows, query))
    norm = lax.rsqrt(jnp.mean(o * o, axis=0, keepdims=True) + EPS)
    eye = lax.broadcasted_iota(jnp.int32, (rows, rows), 0) == lax.broadcasted_iota(jnp.int32, (rows, rows), 1)
    head_gain = jnp.concatenate(
        [jnp.sum(jnp.where(eye, h[...], 0.0), axis=1, keepdims=True) for h in (hg_ref, hg2_ref)], axis=0
    )
    scaled = turned_f32(o * norm * head_gain * gate).astype(BF16)
    columns = out_ref.shape[2]
    for b in range(blocks):
        at = slice(b * columns, (b + 1) * columns)
        w = jnp.concatenate([wo_ref[:, at], wo2_ref[:, at]], axis=0)
        out_ref[b] = mm(scaled, w).astype(BF16)


def sum_kernel(parts_ref, keep_ref, send_ref):
    total = jnp.sum(parts_ref[...].astype(F32), axis=0)
    half = total.shape[1] // 2
    left, right = total[:, :half].astype(BF16), total[:, half:].astype(BF16)
    first = lax.axis_index("tp") == 0
    keep_ref[...] = jnp.where(first, left, right)
    send_ref[...] = jnp.where(first, right, left)


VMEM = pl.BlockSpec(memory_space=pltpu.VMEM)
SMEM = pl.BlockSpec(memory_space=pltpu.SMEM)


def local(
    tokens,
    norm_gain,
    w_query,
    w_key,
    w_value,
    w_gate,
    w_decay,
    w_beta,
    decay_rate,
    head_gain,
    w_out,
    state,
    prev_keys,
    prev_values,
    prev_decay,
    prev_beta,
    accepted,
):
    seqs, steps, lanes = tokens.shape
    half = seqs // 2
    n = half * steps
    rows, features = w_query.shape[1:]
    width = state.shape[-1]
    kv = lax.axis_size("kv")
    tp = lax.axis_index("tp")

    def swapped(a):
        return lax.ppermute(a, "tp", SWAP)

    halves = tokens.reshape(2, n, lanes)
    mine = lax.dynamic_index_in_dim(halves, tp, 0, keepdims=False)
    got = swapped(lax.dynamic_index_in_dim(halves, 1 - tp, 0, keepdims=False))

    mask = (jnp.arange(steps)[None, :] < accepted[:, None]).astype(F32)
    prev_rows = jnp.stack([prev_decay[:, :, 0] * mask, prev_beta[:, :, 0] * mask]).reshape(2, seqs * steps)
    committed, keep, send = pl.pallas_call(
        commit_kernel,
        out_shape=(
            jax.ShapeDtypeStruct((seqs, rows, width), F32),
            jax.ShapeDtypeStruct((half, rows, width), BF16),
            jax.ShapeDtypeStruct((half, rows, width), BF16),
        ),
        in_specs=[VMEM] * 4,
        out_specs=(VMEM,) * 3,
        cost_estimate=pl.CostEstimate(flops=2 * 10**9, bytes_accessed=2 * 10**6, transcendentals=0),
        name="commit",
    )(
        state.reshape(seqs, rows, width),
        prev_keys.reshape(seqs * steps, width),
        prev_values.reshape(seqs * steps, rows),
        prev_rows,
    )
    weights = [w.reshape(rows, features) for w in (w_query, w_key, w_value, w_gate)]
    other = [swapped(w) for w in weights]
    w_own = w_out.reshape(rows, features)
    w_other = swapped(w_own)
    gain = head_gain.reshape(1, rows)
    gain_other = swapped(gain)
    got_state = swapped(send)
    gathered = lax.all_gather(jnp.stack([mine, got]), "kv", axis=0)
    columns = features // kv
    partial = pl.pallas_call(
        layer_kernel,
        out_shape=jax.ShapeDtypeStruct((kv, n, columns), BF16),
        in_specs=[VMEM] * 12 + [SMEM] + [VMEM] * 6,
        out_specs=VMEM,
        cost_estimate=pl.CostEstimate(flops=10**9, bytes_accessed=6 * 10**6, transcendentals=0),
        name="layer",
    )(
        gathered,
        norm_gain.reshape(features // lanes, lanes),
        *weights,
        *other,
        w_decay.T,
        w_beta.T,
        decay_rate,
        gain,
        gain_other,
        keep,
        got_state,
        w_own,
        w_other,
    )
    parts = lax.all_to_all(partial, "kv", split_axis=0, concat_axis=0, tiled=True)
    kept, sent = pl.pallas_call(
        sum_kernel,
        out_shape=(jax.ShapeDtypeStruct((n, columns // 2), BF16),) * 2,
        in_specs=[VMEM],
        out_specs=(VMEM,) * 2,
        name="total",
    )(parts)
    came = swapped(sent)
    mixed = jnp.where(tp == 0, jnp.stack([kept, came]), jnp.stack([came, kept]))
    return mixed.reshape(seqs, steps, lanes), committed.reshape(state.shape)


def solution(mesh):
    in_specs = (
        P(("grp", "dp"), None, ("kv", "tp")),
        P(),
        P("kv", "tp", None),
        P("kv", "tp", None),
        P("kv", "tp", None),
        P("kv", "tp", None),
        P(),
        P(),
        P("kv"),
        P("tp"),
        P("kv", "tp", None),
        P(("grp", "dp"), "kv", "tp", None),
        P(("grp", "dp"), None, "kv", None),
        P(("grp", "dp"), None, "kv", "tp"),
        P(("grp", "dp"), None, "kv"),
        P(("grp", "dp"), None, "kv"),
        P(("grp", "dp")),
    )
    out_specs = (P(("grp", "dp"), None, ("kv", "tp")), P(("grp", "dp"), "kv", "tp", None))
    return jax.shard_map(local, mesh=mesh, in_specs=in_specs, out_specs=out_specs, check_vma=False)
```

```python
import jax
import jax.numpy as jnp
from jax import lax
from jax.experimental import pallas as pl
from jax.experimental.pallas import tpu as pltpu
from jax.sharding import PartitionSpec as P

EPS = 1e-06
F32 = jnp.float32
BF16 = jnp.bfloat16
SWAP = [(0, 1), (1, 0)]


def mm(a, b, dims=((1,), (0,))):
    return lax.dot_general(
        a.astype(BF16), b.astype(BF16), (dims, ((), ())), preferred_element_type=F32
    )


NT = ((1,), (1,))


def high(a, b):
    return lax.dot_general(
        a, b, (((1,), (0,)), ((), ())), precision=lax.Precision.HIGHEST, preferred_element_type=F32
    )


def silu(x):
    return x / (1.0 + jnp.exp(-x))


def turned(x):
    n = x.shape[1]
    eye = lax.broadcasted_iota(jnp.int32, (n, n), 0) == lax.broadcasted_iota(jnp.int32, (n, n), 1)
    return mm(jnp.where(eye, 1.0, 0.0), x, NT)


def decays(d_row, steps):
    n = d_row.shape[1]
    shift = steps.bit_length() - 1
    i = lax.broadcasted_iota(jnp.int32, (n, n), 0)
    r = lax.broadcasted_iota(jnp.int32, (n, n), 1)
    same = (i >> shift) == (r >> shift)
    upto = same & (i <= r)
    before = same & (i < r)
    d_col = jnp.sum(jnp.where(i == r, d_row, 0.0), axis=1, keepdims=True)
    g_row = jnp.sum(jnp.where(upto, d_col, 0.0), axis=0, keepdims=True)
    g_col = jnp.sum(jnp.where(i == r, g_row, 0.0), axis=1, keepdims=True)
    between = jnp.where(upto, jnp.exp(jnp.where(upto, g_row - g_col, 0.0)), 0.0)
    last = jnp.sum(jnp.where(same & ((i & (steps - 1)) == steps - 1), g_col, 0.0), axis=0, keepdims=True)
    return g_row, g_col, last, between, before


def solved(b, n):
    first = b - high(b, n)
    return first + high(first, high(n, n))


def own_products(states, keys_t, seqs, steps):
    product = mm(states, keys_t)
    rows, n = product.shape[0] // seqs, product.shape[1]
    shift = steps.bit_length() - 1
    seq_of = lax.broadcasted_iota(jnp.int32, (rows, n), 1) >> shift
    total = jnp.zeros((rows, n), F32)
    for s in range(seqs):
        total = total + jnp.where(seq_of == s, product[s * rows : (s + 1) * rows], 0.0)
    return total


def commit_kernel(
    state_ref, keys_ref, values_ref, decay_ref, beta_ref, accepted_ref, hg_ref, wq_ref, wk_ref, wv_ref, wg_ref, wo_ref,
    out_ref, pack_ref, weights, states, sent, sems,
):
    seqs, rows, width = state_ref.shape
    steps = decay_ref.shape[0]
    n = seqs * steps
    shift = steps.bit_length() - 1
    count = 5
    loads = [
        pltpu.make_async_copy(w, weights.at[k * rows : (k + 1) * rows], sems.at[k])
        for k, w in enumerate((wq_ref, wk_ref, wv_ref, wg_ref, wo_ref))
    ]
    for load in loads:
        load.start()
    keys = keys_ref[...].astype(F32)
    keys = keys * lax.rsqrt(jnp.sum(keys * keys, axis=-1, keepdims=True) + EPS)
    keys_t = turned_f32(keys)
    step_of = lax.broadcasted_iota(jnp.int32, (steps, n), 1) & (steps - 1)
    own_step = step_of == lax.broadcasted_iota(jnp.int32, (steps, n), 0)
    owner = lax.broadcasted_iota(jnp.int32, (seqs, n), 1) >> shift
    spread = jnp.where(owner == lax.broadcasted_iota(jnp.int32, (seqs, n), 0), 1.0, 0.0)
    taken = high(accepted_ref[...].astype(F32), spread)
    live = jnp.where(step_of[0:1].astype(F32) < taken - 0.5, 1.0, 0.0)
    d_row = -jnp.sum(jnp.where(own_step, high(decay_ref[...], spread), 0.0), axis=0, keepdims=True) * live
    b_row = jnp.sum(jnp.where(own_step, high(beta_ref[...], spread), 0.0), axis=0, keepdims=True) * live
    g_row, g_col, last, between, before = decays(d_row, steps)
    gram = mm(keys, keys, NT)
    nil = jnp.where(before, between * gram * b_row, 0.0)
    state = state_ref[...]
    known = own_products(state.reshape(seqs * rows, width), keys_t, seqs, steps)
    values_t = turned(values_ref[...])
    u = solved(b_row * (values_t - jnp.exp(g_row) * known), nil) * jnp.exp(last - g_row)
    for load in loads:
        load.wait()
    stores = [pltpu.make_async_copy(weights, pack_ref.at[: count * rows], sems.at[count])]
    stores[0].start()
    seq_of = lax.broadcasted_iota(jnp.int32, (rows, n), 1) >> shift
    spread_u = jnp.concatenate([jnp.where(seq_of == s, u, 0.0).astype(BF16) for s in range(seqs)], axis=0)
    update = mm(spread_u, keys)
    kept = jnp.broadcast_to(jnp.exp(g_col), (n, width))
    for s in range(seqs):
        at = s * steps + steps - 1
        states[s] = state[s] * kept[at : at + 1, :] + update[s * rows : (s + 1) * rows]
    half = seqs // 2
    tp = lax.axis_index("tp")
    for s in range(half):
        sent[:, s * width : (s + 1) * width] = states[(1 - tp) * half + s].astype(BF16)
    pieces, rest = [], jnp.concatenate([hg_ref[...], jnp.zeros((1, width - rows), F32)], axis=1)
    for _ in range(3):
        pieces.append(rest.astype(BF16).astype(F32))
        rest = rest - pieces[-1]
    pieces.append(jnp.zeros((rows - 3, width), F32))
    sent[:, half * width :] = jnp.concatenate(pieces, axis=0).astype(BF16)
    stores.append(pltpu.make_async_copy(states, out_ref, sems.at[count + 1]))
    stores[-1].start()
    columns = (half + 1) * width
    stores.append(pltpu.make_async_copy(sent, pack_ref.at[count * rows :, :columns], sems.at[count + 2]))
    stores[-1].start()
    for store in stores:
        store.wait()


def turned_f32(x):
    return turned(x.astype(BF16))


def layer_kernel(
    x_hbm, gain_ref, wq_hbm, wk_hbm, wv_hbm, wg_hbm, decay_hbm, beta_hbm, rate_ref, hg_ref, keep_hbm, wo_hbm, pack_hbm,
    out_ref, same_hbm, x_ref, weights, gates_ref, keep_ref, wo_ref, pack_ref, sems,
):
    blocks, _, n, lanes = x_ref.shape
    seqs, rows, width = keep_ref.shape
    steps = n // seqs
    heads = decay_hbm.shape[0]
    tp = lax.axis_index("tp")
    head = lax.axis_index("kv")
    features = blocks * 2 * lanes
    copies = []

    def fetch(src, dst):
        copies.append(pltpu.make_async_copy(src, dst, sems.at[len(copies)]))
        copies[-1].start()
        return copies[-1]

    x_copy = fetch(x_hbm, x_ref)
    gate_copies = [fetch(decay_hbm, gates_ref.at[:heads]), fetch(beta_hbm, gates_ref.at[heads:])]
    cuts = 4
    cut = features // cuts
    weight_copies = []
    for c in range(cuts):
        at = slice(c * cut, (c + 1) * cut)
        group = [
            fetch(w.at[:, at], weights.at[k * rows : (k + 1) * rows, at])
            for k, w in enumerate((wq_hbm, wk_hbm, wv_hbm, wg_hbm))
        ]
        group.append(fetch(pack_hbm.at[: 4 * rows, at], pack_ref.at[: 4 * rows, at]))
        weight_copies.append(group)
    columns = (seqs + 1) * width
    state_copies = [
        fetch(same_hbm.at[pl.ds(tp * seqs, seqs)], keep_ref),
        fetch(pack_hbm.at[5 * rows :, :columns], pack_ref.at[5 * rows :, :columns]),
    ]
    out_copies = [
        fetch(wo_hbm, wo_ref),
        fetch(pack_hbm.at[4 * rows : 5 * rows], pack_ref.at[4 * rows : 5 * rows]),
    ]
    x_copy.wait()
    squares = jnp.zeros((n, lanes), F32)
    for b in range(blocks):
        for c in range(2):
            part = x_ref[b, c].astype(F32)
            squares = squares + part * part
    scale = lax.rsqrt(jnp.sum(squares, axis=-1, keepdims=True) / features + EPS)
    for copy in gate_copies:
        copy.wait()
    mine = jnp.zeros((4 * rows, n), F32)
    others = jnp.zeros((4 * rows, n), F32)
    gates = jnp.zeros((2 * heads, n), F32)
    for b in range(blocks):
        if b % (blocks // cuts) == 0:
            for copy in weight_copies[b // (blocks // cuts)]:
                copy.wait()
        at = slice(b * 2 * lanes, (b + 1) * 2 * lanes)
        pair = jnp.concatenate([x_ref[b, 0], x_ref[b, 1]], axis=1).astype(F32)
        gain = jnp.concatenate([gain_ref[2 * b : 2 * b + 1, :], gain_ref[2 * b + 1 : 2 * b + 2, :]], axis=1)
        normed = (pair * scale * gain).astype(BF16)
        mine = mine + mm(weights[:, at], normed, NT)
        others = others + mm(pack_ref[: 4 * rows, at], normed, NT)
        gates = gates + mm(gates_ref[:, at], normed, NT)
    for copy in state_copies:
        copy.wait()
    mine = mine.astype(BF16).astype(F32)
    others = others.astype(BF16).astype(F32)

    def in_order(k):
        a, b = mine[k * rows : (k + 1) * rows], others[k * rows : (k + 1) * rows]
        return jnp.where(tp == 0, jnp.concatenate([a, b], axis=0), jnp.concatenate([b, a], axis=0))

    def own_first(k):
        return jnp.concatenate([mine[k * rows : (k + 1) * rows], others[k * rows : (k + 1) * rows]], axis=0)

    def unit(u):
        return u * lax.rsqrt(jnp.sum(u * u, axis=0, keepdims=True) + EPS)

    query = unit(silu(in_order(0))) * width ** (-0.5)
    key = unit(silu(in_order(1)))
    value = silu(own_first(2))
    gate = silu(own_first(3))
    at_head = lax.broadcasted_iota(jnp.int32, (heads, n), 0) == head
    decay_pre = jnp.sum(jnp.where(at_head, gates[:heads], 0.0), axis=0, keepdims=True)
    beta_pre = jnp.sum(jnp.where(at_head, gates[heads:], 0.0), axis=0, keepdims=True)
    softplus = jnp.maximum(decay_pre, 0.0) + jnp.log1p(jnp.exp(-jnp.abs(decay_pre)))
    d_row = -rate_ref[0] * softplus
    b_row = 1.0 / (1.0 + jnp.exp(-beta_pre))
    g_row, _, _, between, before = decays(d_row, steps)

    kept = keep_ref[...].reshape(seqs * rows, width).astype(BF16)
    got = jnp.concatenate([pack_ref[5 * rows :, s * width : (s + 1) * width] for s in range(seqs)], axis=0)

    def from_states(u):
        return jnp.concatenate([own_products(c, u, seqs, steps) for c in (kept, got)], axis=0)

    key_rows = turned_f32(key)
    nil = jnp.where(before, between * mm(key_rows, key) * b_row, 0.0)
    u = solved(b_row * (value - jnp.exp(g_row) * from_states(key)), nil)
    o = jnp.exp(g_row) * from_states(query) + high(u, between * mm(key_rows, query))
    norm = lax.rsqrt(jnp.mean(o * o, axis=0, keepdims=True) + EPS)
    eye = lax.broadcasted_iota(jnp.int32, (rows, rows), 0) == lax.broadcasted_iota(jnp.int32, (rows, rows), 1)
    pieces = pack_ref[5 * rows :, seqs * width : (seqs + 1) * width].astype(F32)[:3, :rows]
    other_gain = pieces[0:1] + pieces[1:2] + pieces[2:3]
    head_gain = jnp.concatenate(
        [jnp.sum(jnp.where(eye, h, 0.0), axis=1, keepdims=True) for h in (hg_ref[...], other_gain)], axis=0
    )
    scaled = turned_f32(o * norm * head_gain * gate).astype(BF16)
    for copy in out_copies:
        copy.wait()
    columns = out_ref.shape[2]
    for b in range(blocks):
        at = slice(b * columns, (b + 1) * columns)
        w = jnp.concatenate([wo_ref[:, at], pack_ref[4 * rows : 5 * rows, at]], axis=0)
        out_ref[b] = mm(scaled, w).astype(BF16)


HBM = pl.BlockSpec(memory_space=pltpu.HBM)
ANY = pl.BlockSpec(memory_space=pl.ANY)
VMEM = pl.BlockSpec(memory_space=pltpu.VMEM)
SMEM = pl.BlockSpec(memory_space=pltpu.SMEM)


def local(
    tokens,
    norm_gain,
    w_query,
    w_key,
    w_value,
    w_gate,
    w_decay,
    w_beta,
    decay_rate,
    head_gain,
    w_out,
    state,
    prev_keys,
    prev_values,
    prev_decay,
    prev_beta,
    accepted,
):
    seqs, steps, lanes = tokens.shape
    half = seqs // 2
    n = half * steps
    rows, features = w_query.shape[1:]
    width = state.shape[-1]
    kv = lax.axis_size("kv")
    tp = lax.axis_index("tp")

    both = lax.all_gather(tokens.reshape(seqs * steps, lanes), "tp", axis=0)
    mine = lax.dynamic_slice_in_dim(both, tp * n, n, 1)
    (both, state) = lax.optimization_barrier((both, state))
    weights = [w.reshape(rows, features) for w in (w_query, w_key, w_value, w_gate)]
    w_own = w_out.reshape(rows, features)
    gain = head_gain.reshape(1, rows)
    committed, pack = pl.pallas_call(
        commit_kernel,
        out_shape=(
            jax.ShapeDtypeStruct((seqs, rows, width), F32),
            jax.ShapeDtypeStruct((6 * rows, features), BF16),
        ),
        in_specs=[VMEM] * 7 + [HBM] * 5,
        out_specs=(HBM, HBM),
        scratch_shapes=[
            pltpu.VMEM((5 * rows, features), BF16),
            pltpu.VMEM((seqs, rows, width), F32),
            pltpu.VMEM((rows, (half + 1) * width), BF16),
            pltpu.SemaphoreType.DMA((8,)),
        ],
        cost_estimate=pl.CostEstimate(flops=2 * 10**9, bytes_accessed=8 * 10**6, transcendentals=0),
        name="commit",
    )(
        state.reshape(seqs, rows, width),
        prev_keys.reshape(seqs * steps, width),
        prev_values.reshape(seqs * steps, rows),
        prev_decay[:, :, 0].T,
        prev_beta[:, :, 0].T,
        accepted.reshape(1, seqs),
        gain,
        *weights,
        w_own,
    )
    pack = lax.ppermute(pack, "tp", SWAP)
    gathered = lax.all_gather(mine, "kv", axis=0)
    columns = features // kv
    partial, committed = pl.pallas_call(
        layer_kernel,
        out_shape=(
            jax.ShapeDtypeStruct((kv, n, columns), BF16),
            jax.ShapeDtypeStruct((seqs, rows, width), F32),
        ),
        input_output_aliases={10: 1},
        in_specs=[ANY, VMEM] + [HBM] * 6 + [SMEM, VMEM, HBM, HBM, ANY],
        out_specs=(VMEM, HBM),
        scratch_shapes=[
            pltpu.VMEM((kv, 2, n, lanes), BF16),
            pltpu.VMEM((4 * rows, features), BF16),
            pltpu.VMEM((2 * w_decay.shape[1], features), BF16),
            pltpu.VMEM((half, rows, width), F32),
            pltpu.VMEM((rows, features), BF16),
            pltpu.VMEM((6 * rows, features), BF16),
            pltpu.SemaphoreType.DMA((32,)),
        ],
        cost_estimate=pl.CostEstimate(flops=10**9, bytes_accessed=6 * 10**6, transcendentals=0),
        compiler_params=pltpu.CompilerParams(vmem_limit_bytes=48 * 2**20),
        name="layer",
    )(
        gathered,
        norm_gain.reshape(features // lanes, lanes),
        *weights,
        w_decay.T,
        w_beta.T,
        decay_rate,
        gain,
        committed,
        w_own,
        pack,
    )
    parts = lax.all_to_all(partial, "kv", split_axis=0, concat_axis=0, tiled=True)
    total = parts.astype(F32).sum(axis=0).astype(BF16)
    mixed = lax.dynamic_slice_in_dim(lax.all_gather(total, "tp", axis=0), tp * lanes, lanes, 2)
    return mixed.reshape(seqs, steps, lanes), committed.reshape(state.shape)


def solution(mesh):
    in_specs = (
        P(("grp", "dp"), None, ("kv", "tp")),
        P(),
        P("kv", "tp", None),
        P("kv", "tp", None),
        P("kv", "tp", None),
        P("kv", "tp", None),
        P(),
        P(),
        P("kv"),
        P("tp"),
        P("kv", "tp", None),
        P(("grp", "dp"), "kv", "tp", None),
        P(("grp", "dp"), None, "kv", None),
        P(("grp", "dp"), None, "kv", "tp"),
        P(("grp", "dp"), None, "kv"),
        P(("grp", "dp"), None, "kv"),
        P(("grp", "dp")),
    )
    out_specs = (P(("grp", "dp"), None, ("kv", "tp")), P(("grp", "dp"), "kv", "tp", None))
    return jax.shard_map(local, mesh=mesh, in_specs=in_specs, out_specs=out_specs, check_vma=False)
```

```python
import jax
import jax.numpy as jnp
from jax import lax
from jax.experimental import pallas as pl
from jax.experimental.pallas import tpu as pltpu
from jax.sharding import PartitionSpec as P

EPS = 1e-06
F32 = jnp.float32
BF16 = jnp.bfloat16
SWAP = [(0, 1), (1, 0)]


def mm(a, b, dims=((1,), (0,))):
    return lax.dot_general(
        a.astype(BF16), b.astype(BF16), (dims, ((), ())), preferred_element_type=F32
    )


NT = ((1,), (1,))


def high(a, b):
    return lax.dot_general(
        a, b, (((1,), (0,)), ((), ())), precision=lax.Precision.HIGHEST, preferred_element_type=F32
    )


def silu(x):
    return x / (1.0 + jnp.exp(-x))


def turned(x):
    n = x.shape[1]
    eye = lax.broadcasted_iota(jnp.int32, (n, n), 0) == lax.broadcasted_iota(jnp.int32, (n, n), 1)
    return mm(jnp.where(eye, 1.0, 0.0), x, NT)


def decays(d_row, steps):
    n = d_row.shape[1]
    shift = steps.bit_length() - 1
    i = lax.broadcasted_iota(jnp.int32, (n, n), 0)
    r = lax.broadcasted_iota(jnp.int32, (n, n), 1)
    same = (i >> shift) == (r >> shift)
    upto = same & (i <= r)
    before = same & (i < r)
    d_col = jnp.sum(jnp.where(i == r, d_row, 0.0), axis=1, keepdims=True)
    g_row = jnp.sum(jnp.where(upto, d_col, 0.0), axis=0, keepdims=True)
    g_col = jnp.sum(jnp.where(i == r, g_row, 0.0), axis=1, keepdims=True)
    between = jnp.where(upto, jnp.exp(jnp.where(upto, g_row - g_col, 0.0)), 0.0)
    last = jnp.sum(jnp.where(same & ((i & (steps - 1)) == steps - 1), g_col, 0.0), axis=0, keepdims=True)
    return g_row, g_col, last, between, before


def solved(b, n):
    first = b - high(b, n)
    return first + high(first, high(n, n))


def own_products(states, keys_t, seqs, steps):
    product = mm(states, keys_t)
    rows, n = product.shape[0] // seqs, product.shape[1]
    shift = steps.bit_length() - 1
    seq_of = lax.broadcasted_iota(jnp.int32, (rows, n), 1) >> shift
    total = jnp.zeros((rows, n), F32)
    for s in range(seqs):
        total = total + jnp.where(seq_of == s, product[s * rows : (s + 1) * rows], 0.0)
    return total


def commit_kernel(
    state_hbm, keys_hbm, values_hbm, decay_hbm, beta_hbm, accepted_hbm, hg_hbm, wq_ref, wk_ref, wv_ref, wg_ref, wo_ref,
    out_ref, pack_ref, state_ref, keys_ref, values_ref, decay_ref, beta_ref, accepted_ref, hg_ref, weights, states, sent, sems,
):
    seqs, rows, width = state_ref.shape
    steps = decay_ref.shape[0]
    n = seqs * steps
    shift = steps.bit_length() - 1
    count = 5
    loads = [
        pltpu.make_async_copy(w, weights.at[k * rows : (k + 1) * rows], sems.at[k])
        for k, w in enumerate((wq_ref, wk_ref, wv_ref, wg_ref, wo_ref))
    ]
    small = [
        pltpu.make_async_copy(a, b, sems.at[count + 3 + k])
        for k, (a, b) in enumerate(
            (
                (keys_hbm, keys_ref),
                (decay_hbm, decay_ref),
                (beta_hbm, beta_ref),
                (accepted_hbm, accepted_ref),
                (values_hbm, values_ref),
                (hg_hbm, hg_ref),
                (state_hbm, state_ref),
            )
        )
    ]
    for load in small + loads:
        load.start()
    for load in small[:-1]:
        load.wait()
    keys = keys_ref[...].astype(F32)
    keys = keys * lax.rsqrt(jnp.sum(keys * keys, axis=-1, keepdims=True) + EPS)
    keys_t = turned_f32(keys)
    step_of = lax.broadcasted_iota(jnp.int32, (steps, n), 1) & (steps - 1)
    own_step = step_of == lax.broadcasted_iota(jnp.int32, (steps, n), 0)
    owner = lax.broadcasted_iota(jnp.int32, (seqs, n), 1) >> shift
    spread = jnp.where(owner == lax.broadcasted_iota(jnp.int32, (seqs, n), 0), 1.0, 0.0)
    taken = high(accepted_ref[...].astype(F32), spread)
    live = jnp.where(step_of[0:1].astype(F32) < taken - 0.5, 1.0, 0.0)
    d_row = -jnp.sum(jnp.where(own_step, high(decay_ref[...], spread), 0.0), axis=0, keepdims=True) * live
    b_row = jnp.sum(jnp.where(own_step, high(beta_ref[...], spread), 0.0), axis=0, keepdims=True) * live
    g_row, g_col, last, between, before = decays(d_row, steps)
    gram = mm(keys, keys, NT)
    nil = jnp.where(before, between * gram * b_row, 0.0)
    small[-1].wait()
    state = state_ref[...]
    known = own_products(state.reshape(seqs * rows, width), keys_t, seqs, steps)
    values_t = turned(values_ref[...])
    for load in loads:
        load.wait()
    stores = [pltpu.make_async_copy(weights, pack_ref.at[: count * rows], sems.at[count])]
    stores[0].start()
    u = solved(b_row * (values_t - jnp.exp(g_row) * known), nil) * jnp.exp(last - g_row)
    seq_of = lax.broadcasted_iota(jnp.int32, (rows, n), 1) >> shift
    spread_u = jnp.concatenate([jnp.where(seq_of == s, u, 0.0).astype(BF16) for s in range(seqs)], axis=0)
    update = mm(spread_u, keys)
    kept = jnp.broadcast_to(jnp.exp(g_col), (n, width))
    for s in range(seqs):
        at = s * steps + steps - 1
        states[s] = state[s] * kept[at : at + 1, :] + update[s * rows : (s + 1) * rows]
    half = seqs // 2
    tp = lax.axis_index("tp")
    for s in range(half):
        sent[:, s * width : (s + 1) * width] = states[(1 - tp) * half + s].astype(BF16)
    pieces, rest = [], jnp.concatenate([hg_ref[...], jnp.zeros((1, width - rows), F32)], axis=1)
    for _ in range(3):
        pieces.append(rest.astype(BF16).astype(F32))
        rest = rest - pieces[-1]
    pieces.append(jnp.zeros((rows - 3, width), F32))
    sent[:, half * width :] = jnp.concatenate(pieces, axis=0).astype(BF16)
    stores.append(pltpu.make_async_copy(states, out_ref, sems.at[count + 1]))
    stores[-1].start()
    columns = (half + 1) * width
    stores.append(pltpu.make_async_copy(sent, pack_ref.at[count * rows :, :columns], sems.at[count + 2]))
    stores[-1].start()
    for store in stores:
        store.wait()


def turned_f32(x):
    return turned(x.astype(BF16))


def layer_kernel(
    x_ref, gain_ref, wq_ref, wk_ref, wv_ref, wg_ref, decay_ref, beta_ref, rate_ref, hg_ref, committed_hbm, wo_ref, pack_hbm,
    out_ref, same_hbm, keep_ref, pack_ref, sems,
):
    blocks, _, n, lanes = x_ref.shape
    seqs, rows, width = keep_ref.shape
    steps = n // seqs
    heads = decay_ref.shape[0]
    tp = lax.axis_index("tp")
    head = lax.axis_index("kv")
    features = blocks * 2 * lanes
    copies = []

    def fetch(src, dst):
        copies.append(pltpu.make_async_copy(src, dst, sems.at[len(copies)]))
        copies[-1].start()
        return copies[-1]

    cuts = 4
    cut = features // cuts
    weight_copies = [
        fetch(pack_hbm.at[: 4 * rows, c * cut : (c + 1) * cut], pack_ref.at[: 4 * rows, c * cut : (c + 1) * cut])
        for c in range(cuts)
    ]
    columns = (seqs + 1) * width
    state_copies = [
        fetch(same_hbm.at[pl.ds(tp * seqs, seqs)], keep_ref),
        fetch(pack_hbm.at[5 * rows :, :columns], pack_ref.at[5 * rows :, :columns]),
    ]
    out_copy = fetch(pack_hbm.at[4 * rows : 5 * rows], pack_ref.at[4 * rows : 5 * rows])
    squares = jnp.zeros((n, lanes), F32)
    for b in range(blocks):
        for c in range(2):
            part = x_ref[b, c].astype(F32)
            squares = squares + part * part
    scale = lax.rsqrt(jnp.sum(squares, axis=-1, keepdims=True) / features + EPS)
    mine = jnp.zeros((4 * rows, n), F32)
    others = jnp.zeros((4 * rows, n), F32)
    gates = jnp.zeros((2 * heads, n), F32)
    for b in range(blocks):
        if b % (blocks // cuts) == 0:
            weight_copies[b // (blocks // cuts)].wait()
        at = slice(b * 2 * lanes, (b + 1) * 2 * lanes)
        pair = jnp.concatenate([x_ref[b, 0], x_ref[b, 1]], axis=1).astype(F32)
        gain = jnp.concatenate([gain_ref[2 * b : 2 * b + 1, :], gain_ref[2 * b + 1 : 2 * b + 2, :]], axis=1)
        normed = (pair * scale * gain).astype(BF16)
        w = jnp.concatenate([r[:, at] for r in (wq_ref, wk_ref, wv_ref, wg_ref)], axis=0)
        mine = mine + mm(w, normed, NT)
        others = others + mm(pack_ref[: 4 * rows, at], normed, NT)
        w = jnp.concatenate([decay_ref[:, at], beta_ref[:, at]], axis=0)
        gates = gates + mm(w, normed, NT)
    for copy in state_copies:
        copy.wait()
    mine = mine.astype(BF16).astype(F32)
    others = others.astype(BF16).astype(F32)

    def in_order(k):
        a, b = mine[k * rows : (k + 1) * rows], others[k * rows : (k + 1) * rows]
        return jnp.where(tp == 0, jnp.concatenate([a, b], axis=0), jnp.concatenate([b, a], axis=0))

    def own_first(k):
        return jnp.concatenate([mine[k * rows : (k + 1) * rows], others[k * rows : (k + 1) * rows]], axis=0)

    def unit(u):
        return u * lax.rsqrt(jnp.sum(u * u, axis=0, keepdims=True) + EPS)

    query = unit(silu(in_order(0))) * width ** (-0.5)
    key = unit(silu(in_order(1)))
    value = silu(own_first(2))
    gate = silu(own_first(3))
    at_head = lax.broadcasted_iota(jnp.int32, (heads, n), 0) == head
    decay_pre = jnp.sum(jnp.where(at_head, gates[:heads], 0.0), axis=0, keepdims=True)
    beta_pre = jnp.sum(jnp.where(at_head, gates[heads:], 0.0), axis=0, keepdims=True)
    softplus = jnp.maximum(decay_pre, 0.0) + jnp.log1p(jnp.exp(-jnp.abs(decay_pre)))
    d_row = -rate_ref[0] * softplus
    b_row = 1.0 / (1.0 + jnp.exp(-beta_pre))
    g_row, _, _, between, before = decays(d_row, steps)

    kept = keep_ref[...].reshape(seqs * rows, width).astype(BF16)
    got = jnp.concatenate([pack_ref[5 * rows :, s * width : (s + 1) * width] for s in range(seqs)], axis=0)

    def from_states(u):
        return jnp.concatenate([own_products(c, u, seqs, steps) for c in (kept, got)], axis=0)

    key_rows = turned_f32(key)
    nil = jnp.where(before, between * mm(key_rows, key) * b_row, 0.0)
    u = solved(b_row * (value - jnp.exp(g_row) * from_states(key)), nil)
    o = jnp.exp(g_row) * from_states(query) + high(u, between * mm(key_rows, query))
    norm = lax.rsqrt(jnp.mean(o * o, axis=0, keepdims=True) + EPS)
    eye = lax.broadcasted_iota(jnp.int32, (rows, rows), 0) == lax.broadcasted_iota(jnp.int32, (rows, rows), 1)
    pieces = pack_ref[5 * rows :, seqs * width : (seqs + 1) * width].astype(F32)[:3, :rows]
    other_gain = pieces[0:1] + pieces[1:2] + pieces[2:3]
    head_gain = jnp.concatenate(
        [jnp.sum(jnp.where(eye, h, 0.0), axis=1, keepdims=True) for h in (hg_ref[...], other_gain)], axis=0
    )
    scaled = turned_f32(o * norm * head_gain * gate).astype(BF16)
    out_copy.wait()
    columns = out_ref.shape[2]
    for b in range(blocks):
        at = slice(b * columns, (b + 1) * columns)
        w = jnp.concatenate([wo_ref[:, at], pack_ref[4 * rows : 5 * rows, at]], axis=0)
        out_ref[b] = mm(scaled, w).astype(BF16)


HBM = pl.BlockSpec(memory_space=pltpu.HBM)
ANY = pl.BlockSpec(memory_space=pl.ANY)
VMEM = pl.BlockSpec(memory_space=pltpu.VMEM)
SMEM = pl.BlockSpec(memory_space=pltpu.SMEM)


def local(
    tokens,
    norm_gain,
    w_query,
    w_key,
    w_value,
    w_gate,
    w_decay,
    w_beta,
    decay_rate,
    head_gain,
    w_out,
    state,
    prev_keys,
    prev_values,
    prev_decay,
    prev_beta,
    accepted,
):
    seqs, steps, lanes = tokens.shape
    half = seqs // 2
    n = half * steps
    rows, features = w_query.shape[1:]
    width = state.shape[-1]
    kv = lax.axis_size("kv")
    tp = lax.axis_index("tp")

    both = lax.all_gather(tokens.reshape(seqs * steps, lanes), "tp", axis=0)
    mine = lax.dynamic_slice_in_dim(both, tp * n, n, 1)
    (both, state) = lax.optimization_barrier((both, state))
    weights = [w.reshape(rows, features) for w in (w_query, w_key, w_value, w_gate)]
    w_own = w_out.reshape(rows, features)
    gain = head_gain.reshape(1, rows)
    committed, pack = pl.pallas_call(
        commit_kernel,
        out_shape=(
            jax.ShapeDtypeStruct((seqs, rows, width), F32),
            jax.ShapeDtypeStruct((6 * rows, features), BF16),
        ),
        in_specs=[HBM] * 12,
        out_specs=(HBM, HBM),
        scratch_shapes=[
            pltpu.VMEM((seqs, rows, width), F32),
            pltpu.VMEM((seqs * steps, width), BF16),
            pltpu.VMEM((seqs * steps, rows), BF16),
            pltpu.VMEM((steps, seqs), F32),
            pltpu.VMEM((steps, seqs), F32),
            pltpu.VMEM((1, seqs), jnp.int32),
            pltpu.VMEM((1, rows), F32),
            pltpu.VMEM((5 * rows, features), BF16),
            pltpu.VMEM((seqs, rows, width), F32),
            pltpu.VMEM((rows, (half + 1) * width), BF16),
            pltpu.SemaphoreType.DMA((16,)),
        ],
        cost_estimate=pl.CostEstimate(flops=2 * 10**9, bytes_accessed=8 * 10**6, transcendentals=0),
        name="commit",
    )(
        state.reshape(seqs, rows, width),
        prev_keys.reshape(seqs * steps, width),
        prev_values.reshape(seqs * steps, rows),
        prev_decay[:, :, 0].T,
        prev_beta[:, :, 0].T,
        accepted.reshape(1, seqs),
        gain,
        *weights,
        w_own,
    )
    pack = lax.ppermute(pack, "tp", SWAP)
    gathered = lax.all_gather(mine, "kv", axis=0)
    columns = features // kv
    partial, committed = pl.pallas_call(
        layer_kernel,
        out_shape=(
            jax.ShapeDtypeStruct((kv, n, columns), BF16),
            jax.ShapeDtypeStruct((seqs, rows, width), F32),
        ),
        input_output_aliases={10: 1},
        in_specs=[VMEM] * 8 + [SMEM, VMEM, HBM, VMEM, HBM],
        out_specs=(VMEM, HBM),
        scratch_shapes=[
            pltpu.VMEM((half, rows, width), F32),
            pltpu.VMEM((6 * rows, features), BF16),
            pltpu.SemaphoreType.DMA((8,)),
        ],
        cost_estimate=pl.CostEstimate(flops=10**9, bytes_accessed=6 * 10**6, transcendentals=0),
        compiler_params=pltpu.CompilerParams(vmem_limit_bytes=48 * 2**20),
        name="layer",
    )(
        gathered,
        norm_gain.reshape(features // lanes, lanes),
        *weights,
        w_decay.T,
        w_beta.T,
        decay_rate,
        gain,
        committed,
        w_own,
        pack,
    )
    parts = lax.all_to_all(partial, "kv", split_axis=0, concat_axis=0, tiled=True)
    total = parts.astype(F32).sum(axis=0).astype(BF16)
    mixed = lax.dynamic_slice_in_dim(lax.all_gather(total, "tp", axis=0), tp * lanes, lanes, 2)
    return mixed.reshape(seqs, steps, lanes), committed.reshape(state.shape)


def solution(mesh):
    in_specs = (
        P(("grp", "dp"), None, ("kv", "tp")),
        P(),
        P("kv", "tp", None),
        P("kv", "tp", None),
        P("kv", "tp", None),
        P("kv", "tp", None),
        P(),
        P(),
        P("kv"),
        P("tp"),
        P("kv", "tp", None),
        P(("grp", "dp"), "kv", "tp", None),
        P(("grp", "dp"), None, "kv", None),
        P(("grp", "dp"), None, "kv", "tp"),
        P(("grp", "dp"), None, "kv"),
        P(("grp", "dp"), None, "kv"),
        P(("grp", "dp")),
    )
    out_specs = (P(("grp", "dp"), None, ("kv", "tp")), P(("grp", "dp"), "kv", "tp", None))
    return jax.shard_map(local, mesh=mesh, in_specs=in_specs, out_specs=out_specs, check_vma=False)
```

```python
import jax
import jax.numpy as jnp
from jax import lax
from jax.experimental import pallas as pl
from jax.experimental.pallas import tpu as pltpu
from jax.sharding import PartitionSpec as P


EPS = 1e-06
F32 = jnp.float32
BF16 = jnp.bfloat16
SWAP = [(0, 1), (1, 0)]


def mm(a, b, dims=((1,), (0,))):
    return lax.dot_general(
        a.astype(BF16), b.astype(BF16), (dims, ((), ())), preferred_element_type=F32
    )


NT = ((1,), (1,))


def high(a, b):
    return lax.dot_general(
        a, b, (((1,), (0,)), ((), ())), precision=lax.Precision.HIGHEST, preferred_element_type=F32
    )


def silu(x):
    return x / (1.0 + jnp.exp(-x))


def turned(x):
    n = x.shape[1]
    eye = lax.broadcasted_iota(jnp.int32, (n, n), 0) == lax.broadcasted_iota(jnp.int32, (n, n), 1)
    return mm(jnp.where(eye, 1.0, 0.0), x, NT)


def decays(d_row, steps):
    n = d_row.shape[1]
    shift = steps.bit_length() - 1
    i = lax.broadcasted_iota(jnp.int32, (n, n), 0)
    r = lax.broadcasted_iota(jnp.int32, (n, n), 1)
    same = (i >> shift) == (r >> shift)
    upto = same & (i <= r)
    before = same & (i < r)
    d_col = jnp.sum(jnp.where(i == r, d_row, 0.0), axis=1, keepdims=True)
    g_row = jnp.sum(jnp.where(upto, d_col, 0.0), axis=0, keepdims=True)
    g_col = jnp.sum(jnp.where(i == r, g_row, 0.0), axis=1, keepdims=True)
    between = jnp.where(upto, jnp.exp(jnp.where(upto, g_row - g_col, 0.0)), 0.0)
    last = jnp.sum(jnp.where(same & ((i & (steps - 1)) == steps - 1), g_col, 0.0), axis=0, keepdims=True)
    return g_row, g_col, last, between, before


def inverse(n):
    eye = lax.broadcasted_iota(jnp.int32, n.shape, 0) == lax.broadcasted_iota(jnp.int32, n.shape, 1)
    square = high(n, n)
    return jnp.where(eye, 1.0, 0.0) - n + square - high(n, square)


def own_products(states, keys_t, seqs, steps):
    product = mm(states, keys_t)
    rows, n = product.shape[0] // seqs, product.shape[1]
    shift = steps.bit_length() - 1
    seq_of = lax.broadcasted_iota(jnp.int32, (rows, n), 1) >> shift
    total = jnp.zeros((rows, n), F32)
    for s in range(seqs):
        total = total + jnp.where(seq_of == s, product[s * rows : (s + 1) * rows], 0.0)
    return total


def commit_kernel(
    state_hbm, keys_hbm, values_hbm, decay_hbm, beta_hbm, accepted_hbm, hg_hbm, wq_ref, wk_ref, wv_ref, wg_ref, wo_ref,
    out_ref, pack_ref, state_ref, keys_ref, values_ref, decay_ref, beta_ref, accepted_ref, hg_ref, weights, states, sent, sems,
):
    seqs, rows, width = state_ref.shape
    steps = decay_ref.shape[0]
    n = seqs * steps
    shift = steps.bit_length() - 1
    count = 5
    loads = [
        pltpu.make_async_copy(w, weights.at[k * rows : (k + 1) * rows], sems.at[k])
        for k, w in enumerate((wq_ref, wk_ref, wv_ref, wg_ref, wo_ref))
    ]
    small = [
        pltpu.make_async_copy(a, b, sems.at[count + 3 + k])
        for k, (a, b) in enumerate(
            (
                (keys_hbm, keys_ref),
                (decay_hbm, decay_ref),
                (beta_hbm, beta_ref),
                (accepted_hbm, accepted_ref),
                (values_hbm, values_ref),
                (hg_hbm, hg_ref),
                (state_hbm, state_ref),
            )
        )
    ]
    for load in small + loads:
        load.start()
    for load in small[:-1]:
        load.wait()
    keys = keys_ref[...].astype(F32)
    keys = keys * lax.rsqrt(jnp.sum(keys * keys, axis=-1, keepdims=True) + EPS)
    keys_t = turned_f32(keys)
    step_of = lax.broadcasted_iota(jnp.int32, (steps, n), 1) & (steps - 1)
    own_step = step_of == lax.broadcasted_iota(jnp.int32, (steps, n), 0)
    owner = lax.broadcasted_iota(jnp.int32, (seqs, n), 1) >> shift
    spread = jnp.where(owner == lax.broadcasted_iota(jnp.int32, (seqs, n), 0), 1.0, 0.0)
    taken = high(accepted_ref[...].astype(F32), spread)
    live = jnp.where(step_of[0:1].astype(F32) < taken - 0.5, 1.0, 0.0)
    d_row = -jnp.sum(jnp.where(own_step, high(decay_ref[...], spread), 0.0), axis=0, keepdims=True) * live
    b_row = jnp.sum(jnp.where(own_step, high(beta_ref[...], spread), 0.0), axis=0, keepdims=True) * live
    g_row, g_col, last, between, before = decays(d_row, steps)
    gram = mm(keys, keys, NT)
    nil = jnp.where(before, between * gram * b_row, 0.0)
    back = inverse(nil)
    values_t = turned(values_ref[...])
    small[-1].wait()
    state = state_ref[...]
    known = own_products(state.reshape(seqs * rows, width), keys_t, seqs, steps)
    stores = []
    for k, load in enumerate(loads):
        at = slice(k * rows, (k + 1) * rows)
        load.wait()
        stores.append(pltpu.make_async_copy(weights.at[at], pack_ref.at[at], sems.at[count + 10 + k]))
        stores[-1].start()
    u = high(b_row * (values_t - jnp.exp(g_row) * known), back) * jnp.exp(last - g_row)
    seq_of = lax.broadcasted_iota(jnp.int32, (rows, n), 1) >> shift
    spread_u = jnp.concatenate([jnp.where(seq_of == s, u, 0.0).astype(BF16) for s in range(seqs)], axis=0)
    update = mm(spread_u, keys)
    kept = jnp.broadcast_to(jnp.exp(g_col), (n, width))
    for s in range(seqs):
        at = s * steps + steps - 1
        states[s] = state[s] * kept[at : at + 1, :] + update[s * rows : (s + 1) * rows]
    half = seqs // 2
    tp = lax.axis_index("tp")
    for s in range(half):
        sent[:, s * width : (s + 1) * width] = states[(1 - tp) * half + s].astype(BF16)
    pieces, rest = [], jnp.concatenate([hg_ref[...], jnp.zeros((1, width - rows), F32)], axis=1)
    for _ in range(3):
        pieces.append(rest.astype(BF16).astype(F32))
        rest = rest - pieces[-1]
    pieces.append(jnp.zeros((rows - 3, width), F32))
    sent[:, half * width :] = jnp.concatenate(pieces, axis=0).astype(BF16)
    stores.append(pltpu.make_async_copy(states, out_ref, sems.at[count + 1]))
    stores[-1].start()
    columns = (half + 1) * width
    stores.append(pltpu.make_async_copy(sent, pack_ref.at[count * rows :, :columns], sems.at[count + 2]))
    stores[-1].start()
    for store in stores:
        store.wait()


def turned_f32(x):
    return turned(x.astype(BF16))


def layer_kernel(
    x_ref, gain_ref, wq_ref, wk_ref, wv_ref, wg_ref, decay_ref, beta_ref, rate_ref, hg_ref, committed_hbm, wo_ref, pack_hbm,
    out_ref, same_hbm, keep_ref, pack_ref, sems,
):
    _, blocks, all_rows, lanes = x_ref.shape
    n = all_rows // 2
    seqs, rows, width = keep_ref.shape
    steps = n // seqs
    heads = decay_ref.shape[0]
    tp = lax.axis_index("tp")
    head = lax.axis_index("kv")
    features = blocks * 2 * lanes
    copies = []

    def fetch(src, dst):
        copies.append(pltpu.make_async_copy(src, dst, sems.at[len(copies)]))
        copies[-1].start()
        return copies[-1]

    cuts = 4
    cut = features // cuts
    weight_copies = [
        fetch(pack_hbm.at[: 4 * rows, c * cut : (c + 1) * cut], pack_ref.at[: 4 * rows, c * cut : (c + 1) * cut])
        for c in range(cuts)
    ]
    columns = (seqs + 1) * width
    state_copies = [
        fetch(same_hbm.at[pl.ds(tp * seqs, seqs)], keep_ref),
        fetch(pack_hbm.at[5 * rows :, :columns], pack_ref.at[5 * rows :, :columns]),
    ]
    out_copy = fetch(pack_hbm.at[4 * rows : 5 * rows], pack_ref.at[4 * rows : 5 * rows])
    own_rows = pl.ds(pl.multiple_of(tp * n, n), n)
    squares = jnp.zeros((n, lanes), F32)
    for b in range(blocks):
        for c in range(2):
            part = x_ref[c, b, own_rows, :].astype(F32)
            squares = squares + part * part
    scale = lax.rsqrt(jnp.sum(squares, axis=-1, keepdims=True) / features + EPS)
    mine = jnp.zeros((4 * rows, n), F32)
    others = jnp.zeros((4 * rows, n), F32)
    gates = jnp.zeros((2 * heads, n), F32)
    for b in range(blocks):
        if b % (blocks // cuts) == 0:
            weight_copies[b // (blocks // cuts)].wait()
        at = slice(b * 2 * lanes, (b + 1) * 2 * lanes)
        pair = jnp.concatenate([x_ref[c, b, own_rows, :] for c in range(2)], axis=1).astype(F32)
        gain = jnp.concatenate([gain_ref[2 * b : 2 * b + 1, :], gain_ref[2 * b + 1 : 2 * b + 2, :]], axis=1)
        normed = (pair * scale * gain).astype(BF16)
        w = jnp.concatenate([r[:, at] for r in (wq_ref, wk_ref, wv_ref, wg_ref)], axis=0)
        mine = mine + mm(w, normed, NT)
        others = others + mm(pack_ref[: 4 * rows, at], normed, NT)
        w = jnp.concatenate([decay_ref[:, at], beta_ref[:, at]], axis=0)
        gates = gates + mm(w, normed, NT)
    for copy in state_copies:
        copy.wait()
    mine = mine.astype(BF16).astype(F32)
    others = others.astype(BF16).astype(F32)

    def in_order(k):
        a, b = mine[k * rows : (k + 1) * rows], others[k * rows : (k + 1) * rows]
        return jnp.where(tp == 0, jnp.concatenate([a, b], axis=0), jnp.concatenate([b, a], axis=0))

    def own_first(k):
        return jnp.concatenate([mine[k * rows : (k + 1) * rows], others[k * rows : (k + 1) * rows]], axis=0)

    def unit(u):
        return u * lax.rsqrt(jnp.sum(u * u, axis=0, keepdims=True) + EPS)

    query = unit(silu(in_order(0))) * width ** (-0.5)
    key = unit(silu(in_order(1)))
    value = silu(own_first(2))
    gate = silu(own_first(3))
    at_head = lax.broadcasted_iota(jnp.int32, (heads, n), 0) == head
    decay_pre = jnp.sum(jnp.where(at_head, gates[:heads], 0.0), axis=0, keepdims=True)
    beta_pre = jnp.sum(jnp.where(at_head, gates[heads:], 0.0), axis=0, keepdims=True)
    softplus = jnp.maximum(decay_pre, 0.0) + jnp.log1p(jnp.exp(-jnp.abs(decay_pre)))
    d_row = -rate_ref[0] * softplus
    b_row = 1.0 / (1.0 + jnp.exp(-beta_pre))
    g_row, _, _, between, before = decays(d_row, steps)

    kept = keep_ref[...].reshape(seqs * rows, width).astype(BF16)
    got = jnp.concatenate([pack_ref[5 * rows :, s * width : (s + 1) * width] for s in range(seqs)], axis=0)

    def from_states(u):
        return jnp.concatenate([own_products(c, u, seqs, steps) for c in (kept, got)], axis=0)

    key_rows = turned_f32(key)
    nil = jnp.where(before, between * mm(key_rows, key) * b_row, 0.0)
    back = inverse(nil)
    u = high(b_row * (value - jnp.exp(g_row) * from_states(key)), back)
    o = jnp.exp(g_row) * from_states(query) + high(u, between * mm(key_rows, query))
    norm = lax.rsqrt(jnp.mean(o * o, axis=0, keepdims=True) + EPS)
    eye = lax.broadcasted_iota(jnp.int32, (rows, rows), 0) == lax.broadcasted_iota(jnp.int32, (rows, rows), 1)
    pieces = pack_ref[5 * rows :, seqs * width : (seqs + 1) * width].astype(F32)[:3, :rows]
    other_gain = pieces[0:1] + pieces[1:2] + pieces[2:3]
    head_gain = jnp.concatenate(
        [jnp.sum(jnp.where(eye, h, 0.0), axis=1, keepdims=True) for h in (hg_ref[...], other_gain)], axis=0
    )
    scaled = turned_f32(o * norm * head_gain * gate).astype(BF16)
    out_copy.wait()
    columns = out_ref.shape[2]
    for b in range(blocks):
        at = slice(b * columns, (b + 1) * columns)
        w = jnp.concatenate([wo_ref[:, at], pack_ref[4 * rows : 5 * rows, at]], axis=0)
        out_ref[b] = mm(scaled, w).astype(BF16)


HBM = pl.BlockSpec(memory_space=pltpu.HBM)
ANY = pl.BlockSpec(memory_space=pl.ANY)
VMEM = pl.BlockSpec(memory_space=pltpu.VMEM)
SMEM = pl.BlockSpec(memory_space=pltpu.SMEM)


def local(
    tokens,
    norm_gain,
    w_query,
    w_key,
    w_value,
    w_gate,
    w_decay,
    w_beta,
    decay_rate,
    head_gain,
    w_out,
    state,
    prev_keys,
    prev_values,
    prev_decay,
    prev_beta,
    accepted,
):
    seqs, steps, lanes = tokens.shape
    half = seqs // 2
    n = half * steps
    rows, features = w_query.shape[1:]
    width = state.shape[-1]
    kv = lax.axis_size("kv")
    tp = lax.axis_index("tp")

    copies = jnp.broadcast_to(tokens.reshape(1, seqs * steps, lanes), (kv, seqs * steps, lanes))
    ours = lax.all_to_all(copies, "kv", split_axis=0, concat_axis=0, tiled=True)
    weights = [w.reshape(rows, features) for w in (w_query, w_key, w_value, w_gate)]
    w_own = w_out.reshape(rows, features)
    gain = head_gain.reshape(1, rows)
    commit = pl.pallas_call(
        commit_kernel,
        out_shape=(
            jax.ShapeDtypeStruct((seqs, rows, width), F32),
            jax.ShapeDtypeStruct((6 * rows, features), BF16),
        ),
        in_specs=[HBM] * 12,
        out_specs=(HBM, HBM),
        scratch_shapes=[
            pltpu.VMEM((seqs, rows, width), F32),
            pltpu.VMEM((seqs * steps, width), BF16),
            pltpu.VMEM((seqs * steps, rows), BF16),
            pltpu.VMEM((steps, seqs), F32),
            pltpu.VMEM((steps, seqs), F32),
            pltpu.VMEM((1, seqs), jnp.int32),
            pltpu.VMEM((1, rows), F32),
            pltpu.VMEM((5 * rows, features), BF16),
            pltpu.VMEM((seqs, rows, width), F32),
            pltpu.VMEM((rows, (half + 1) * width), BF16),
            pltpu.SemaphoreType.DMA((20,)),
        ],
        cost_estimate=pl.CostEstimate(flops=2 * 10**9, bytes_accessed=8 * 10**6, transcendentals=0),
        name="commit",
    )
    committed, pack = commit(
        state.reshape(seqs, rows, width),
        prev_keys.reshape(seqs * steps, width),
        prev_values.reshape(seqs * steps, rows),
        prev_decay[:, :, 0].T,
        prev_beta[:, :, 0].T,
        accepted.reshape(1, seqs),
        gain,
        *weights,
        w_own,
    )
    pack = lax.ppermute(pack, "tp", SWAP)
    gathered = lax.all_gather(ours, "tp", axis=0)
    columns = features // kv
    partial, committed = pl.pallas_call(
        layer_kernel,
        out_shape=(
            jax.ShapeDtypeStruct((kv, n, columns), BF16),
            jax.ShapeDtypeStruct((seqs, rows, width), F32),
        ),
        input_output_aliases={10: 1},
        in_specs=[VMEM] * 8 + [SMEM, VMEM, HBM, VMEM, HBM],
        out_specs=(VMEM, HBM),
        scratch_shapes=[
            pltpu.VMEM((half, rows, width), F32),
            pltpu.VMEM((6 * rows, features), BF16),
            pltpu.SemaphoreType.DMA((8,)),
        ],
        cost_estimate=pl.CostEstimate(flops=10**9, bytes_accessed=6 * 10**6, transcendentals=0),
        compiler_params=pltpu.CompilerParams(vmem_limit_bytes=48 * 2**20),
        name="layer",
    )(
        gathered,
        norm_gain.reshape(features // lanes, lanes),
        *weights,
        w_decay.T,
        w_beta.T,
        decay_rate,
        gain,
        committed,
        w_own,
        pack,
    )
    parts = lax.all_to_all(partial, "kv", split_axis=0, concat_axis=0, tiled=True)
    total = parts.astype(F32).sum(axis=0).astype(BF16)
    mixed = lax.dynamic_slice_in_dim(lax.all_gather(total, "tp", axis=0), tp * lanes, lanes, 2)
    return mixed.reshape(seqs, steps, lanes), committed.reshape(state.shape)


def solution(mesh):
    in_specs = (
        P(("grp", "dp"), None, ("kv", "tp")),
        P(),
        P("kv", "tp", None),
        P("kv", "tp", None),
        P("kv", "tp", None),
        P("kv", "tp", None),
        P(),
        P(),
        P("kv"),
        P("tp"),
        P("kv", "tp", None),
        P(("grp", "dp"), "kv", "tp", None),
        P(("grp", "dp"), None, "kv", None),
        P(("grp", "dp"), None, "kv", "tp"),
        P(("grp", "dp"), None, "kv"),
        P(("grp", "dp"), None, "kv"),
        P(("grp", "dp")),
    )
    out_specs = (P(("grp", "dp"), None, ("kv", "tp")), P(("grp", "dp"), "kv", "tp", None))
    return jax.shard_map(local, mesh=mesh, in_specs=in_specs, out_specs=out_specs, check_vma=False)
```

```python
import jax
import jax.numpy as jnp
from jax import lax
from jax.experimental import pallas as pl
from jax.experimental.pallas import tpu as pltpu
from jax.sharding import PartitionSpec as P


EPS = 1e-06
F32 = jnp.float32
BF16 = jnp.bfloat16
SWAP = [(0, 1), (1, 0)]


def mm(a, b, dims=((1,), (0,))):
    return lax.dot_general(
        a.astype(BF16), b.astype(BF16), (dims, ((), ())), preferred_element_type=F32
    )


NT = ((1,), (1,))


def high(a, b):
    return lax.dot_general(
        a, b, (((1,), (0,)), ((), ())), precision=lax.Precision.HIGHEST, preferred_element_type=F32
    )


def silu(x):
    return x / (1.0 + jnp.exp(-x))


def turned(x):
    n = x.shape[1]
    eye = lax.broadcasted_iota(jnp.int32, (n, n), 0) == lax.broadcasted_iota(jnp.int32, (n, n), 1)
    return mm(jnp.where(eye, 1.0, 0.0), x, NT)


def decays(d_row, steps):
    n = d_row.shape[1]
    shift = steps.bit_length() - 1
    i = lax.broadcasted_iota(jnp.int32, (n, n), 0)
    r = lax.broadcasted_iota(jnp.int32, (n, n), 1)
    same = (i >> shift) == (r >> shift)
    upto = same & (i <= r)
    before = same & (i < r)
    d_col = jnp.sum(jnp.where(i == r, d_row, 0.0), axis=1, keepdims=True)
    g_row = jnp.sum(jnp.where(upto, d_col, 0.0), axis=0, keepdims=True)
    g_col = jnp.sum(jnp.where(i == r, g_row, 0.0), axis=1, keepdims=True)
    between = jnp.where(upto, jnp.exp(jnp.where(upto, g_row - g_col, 0.0)), 0.0)
    last = jnp.sum(jnp.where(same & ((i & (steps - 1)) == steps - 1), g_col, 0.0), axis=0, keepdims=True)
    return g_row, g_col, last, between, before


def inverse(n):
    eye = lax.broadcasted_iota(jnp.int32, n.shape, 0) == lax.broadcasted_iota(jnp.int32, n.shape, 1)
    square = high(n, n)
    return jnp.where(eye, 1.0, 0.0) - n + square - high(n, square)


def own_products(states, keys_t, seqs, steps):
    product = mm(states, keys_t)
    rows, n = product.shape[0] // seqs, product.shape[1]
    shift = steps.bit_length() - 1
    seq_of = lax.broadcasted_iota(jnp.int32, (rows, n), 1) >> shift
    total = jnp.zeros((rows, n), F32)
    for s in range(seqs):
        total = total + jnp.where(seq_of == s, product[s * rows : (s + 1) * rows], 0.0)
    return total


def commit_kernel(
    state_hbm, keys_hbm, values_hbm, decay_hbm, beta_hbm, accepted_hbm, hg_hbm, wq_ref, wk_ref, wv_ref, wg_ref, wo_ref,
    out_ref, pack_ref, state_ref, keys_ref, values_ref, decay_ref, beta_ref, accepted_ref, hg_ref, weights, states, sent, sems,
):
    seqs, rows, width = state_ref.shape
    steps = decay_ref.shape[0]
    n = seqs * steps
    shift = steps.bit_length() - 1
    count = 5
    loads = [
        pltpu.make_async_copy(w, weights.at[k * rows : (k + 1) * rows], sems.at[k])
        for k, w in enumerate((wq_ref, wk_ref, wv_ref, wg_ref, wo_ref))
    ]
    small = [
        pltpu.make_async_copy(a, b, sems.at[count + 3 + k])
        for k, (a, b) in enumerate(
            (
                (keys_hbm, keys_ref),
                (decay_hbm, decay_ref),
                (beta_hbm, beta_ref),
                (accepted_hbm, accepted_ref),
                (values_hbm, values_ref),
                (hg_hbm, hg_ref),
                (state_hbm, state_ref),
            )
        )
    ]
    for load in small + loads:
        load.start()
    for load in small[:-1]:
        load.wait()
    keys = keys_ref[...].astype(F32)
    keys = keys * lax.rsqrt(jnp.sum(keys * keys, axis=-1, keepdims=True) + EPS)
    keys_t = turned_f32(keys)
    step_of = lax.broadcasted_iota(jnp.int32, (steps, n), 1) & (steps - 1)
    own_step = step_of == lax.broadcasted_iota(jnp.int32, (steps, n), 0)
    owner = lax.broadcasted_iota(jnp.int32, (seqs, n), 1) >> shift
    spread = jnp.where(owner == lax.broadcasted_iota(jnp.int32, (seqs, n), 0), 1.0, 0.0)
    taken = high(accepted_ref[...].astype(F32), spread)
    live = jnp.where(step_of[0:1].astype(F32) < taken - 0.5, 1.0, 0.0)
    d_row = -jnp.sum(jnp.where(own_step, high(decay_ref[...], spread), 0.0), axis=0, keepdims=True) * live
    b_row = jnp.sum(jnp.where(own_step, high(beta_ref[...], spread), 0.0), axis=0, keepdims=True) * live
    g_row, g_col, last, between, before = decays(d_row, steps)
    gram = mm(keys, keys, NT)
    nil = jnp.where(before, between * gram * b_row, 0.0)
    back = inverse(nil)
    values_t = turned(values_ref[...])
    small[-1].wait()
    state = state_ref[...]
    known = own_products(state.reshape(seqs * rows, width), keys_t, seqs, steps)
    stores = []
    for k, load in enumerate(loads):
        at = slice(k * rows, (k + 1) * rows)
        load.wait()
        stores.append(pltpu.make_async_copy(weights.at[at], pack_ref.at[at], sems.at[count + 10 + k]))
        stores[-1].start()
    u = high(b_row * (values_t - jnp.exp(g_row) * known), back) * jnp.exp(last - g_row)
    seq_of = lax.broadcasted_iota(jnp.int32, (rows, n), 1) >> shift
    spread_u = jnp.concatenate([jnp.where(seq_of == s, u, 0.0).astype(BF16) for s in range(seqs)], axis=0)
    update = mm(spread_u, keys)
    kept = jnp.broadcast_to(jnp.exp(g_col), (n, width))
    for s in range(seqs):
        at = s * steps + steps - 1
        states[s] = state[s] * kept[at : at + 1, :] + update[s * rows : (s + 1) * rows]
    half = seqs // 2
    tp = lax.axis_index("tp")
    for s in range(half):
        sent[:, s * width : (s + 1) * width] = states[(1 - tp) * half + s].astype(BF16)
    pieces, rest = [], jnp.concatenate([hg_ref[...], jnp.zeros((1, width - rows), F32)], axis=1)
    for _ in range(3):
        pieces.append(rest.astype(BF16).astype(F32))
        rest = rest - pieces[-1]
    pieces.append(jnp.zeros((rows - 3, width), F32))
    sent[:, half * width :] = jnp.concatenate(pieces, axis=0).astype(BF16)
    stores.append(pltpu.make_async_copy(states, out_ref, sems.at[count + 1]))
    stores[-1].start()
    columns = (half + 1) * width
    stores.append(pltpu.make_async_copy(sent, pack_ref.at[count * rows :, :columns], sems.at[count + 2]))
    stores[-1].start()
    for store in stores:
        store.wait()


def turned_f32(x):
    return turned(x.astype(BF16))


def layer_kernel(
    x_ref, gain_ref, wq_ref, wk_ref, wv_ref, wg_ref, decay_ref, beta_ref, rate_ref, hg_ref, committed_hbm, wo_ref, pack_hbm,
    out_ref, same_hbm, keep_ref, pack_ref, sems,
):
    blocks, _, n, lanes = x_ref.shape
    seqs, rows, width = keep_ref.shape
    steps = n // seqs
    heads = decay_ref.shape[0]
    tp = lax.axis_index("tp")
    head = lax.axis_index("kv")
    features = blocks * 2 * lanes
    copies = []

    def fetch(src, dst):
        copies.append(pltpu.make_async_copy(src, dst, sems.at[len(copies)]))
        copies[-1].start()
        return copies[-1]

    cuts = 4
    cut = features // cuts
    weight_copies = [
        fetch(pack_hbm.at[: 4 * rows, c * cut : (c + 1) * cut], pack_ref.at[: 4 * rows, c * cut : (c + 1) * cut])
        for c in range(cuts)
    ]
    columns = (seqs + 1) * width
    state_copies = [
        fetch(same_hbm.at[pl.ds(tp * seqs, seqs)], keep_ref),
        fetch(pack_hbm.at[5 * rows :, :columns], pack_ref.at[5 * rows :, :columns]),
    ]
    out_copy = fetch(pack_hbm.at[4 * rows : 5 * rows], pack_ref.at[4 * rows : 5 * rows])
    squares = jnp.zeros((n, lanes), F32)
    for b in range(blocks):
        for c in range(2):
            part = x_ref[b, c].astype(F32)
            squares = squares + part * part
    scale = lax.rsqrt(jnp.sum(squares, axis=-1, keepdims=True) / features + EPS)
    mine = jnp.zeros((4 * rows, n), F32)
    others = jnp.zeros((4 * rows, n), F32)
    gates = jnp.zeros((2 * heads, n), F32)
    for b in range(blocks):
        if b % (blocks // cuts) == 0:
            weight_copies[b // (blocks // cuts)].wait()
        at = slice(b * 2 * lanes, (b + 1) * 2 * lanes)
        pair = jnp.concatenate([x_ref[b, 0], x_ref[b, 1]], axis=1).astype(F32)
        gain = jnp.concatenate([gain_ref[2 * b : 2 * b + 1, :], gain_ref[2 * b + 1 : 2 * b + 2, :]], axis=1)
        normed = (pair * scale * gain).astype(BF16)
        w = jnp.concatenate([r[:, at] for r in (wq_ref, wk_ref, wv_ref, wg_ref)], axis=0)
        mine = mine + mm(w, normed, NT)
        others = others + mm(pack_ref[: 4 * rows, at], normed, NT)
        w = jnp.concatenate([decay_ref[:, at], beta_ref[:, at]], axis=0)
        gates = gates + mm(w, normed, NT)
    for copy in state_copies:
        copy.wait()
    mine = mine.astype(BF16).astype(F32)
    others = others.astype(BF16).astype(F32)

    def in_order(k):
        a, b = mine[k * rows : (k + 1) * rows], others[k * rows : (k + 1) * rows]
        return jnp.where(tp == 0, jnp.concatenate([a, b], axis=0), jnp.concatenate([b, a], axis=0))

    def own_first(k):
        return jnp.concatenate([mine[k * rows : (k + 1) * rows], others[k * rows : (k + 1) * rows]], axis=0)

    def unit(u):
        return u * lax.rsqrt(jnp.sum(u * u, axis=0, keepdims=True) + EPS)

    query = unit(silu(in_order(0))) * width ** (-0.5)
    key = unit(silu(in_order(1)))
    value = silu(own_first(2))
    gate = silu(own_first(3))
    at_head = lax.broadcasted_iota(jnp.int32, (heads, n), 0) == head
    decay_pre = jnp.sum(jnp.where(at_head, gates[:heads], 0.0), axis=0, keepdims=True)
    beta_pre = jnp.sum(jnp.where(at_head, gates[heads:], 0.0), axis=0, keepdims=True)
    softplus = jnp.maximum(decay_pre, 0.0) + jnp.log1p(jnp.exp(-jnp.abs(decay_pre)))
    d_row = -rate_ref[0] * softplus
    b_row = 1.0 / (1.0 + jnp.exp(-beta_pre))
    g_row, _, _, between, before = decays(d_row, steps)

    kept = keep_ref[...].reshape(seqs * rows, width).astype(BF16)
    got = jnp.concatenate([pack_ref[5 * rows :, s * width : (s + 1) * width] for s in range(seqs)], axis=0)

    def from_states(u):
        return jnp.concatenate([own_products(c, u, seqs, steps) for c in (kept, got)], axis=0)

    key_rows = turned_f32(key)
    nil = jnp.where(before, between * mm(key_rows, key) * b_row, 0.0)
    back = inverse(nil)
    u = high(b_row * (value - jnp.exp(g_row) * from_states(key)), back)
    o = jnp.exp(g_row) * from_states(query) + high(u, between * mm(key_rows, query))
    norm = lax.rsqrt(jnp.mean(o * o, axis=0, keepdims=True) + EPS)
    eye = lax.broadcasted_iota(jnp.int32, (rows, rows), 0) == lax.broadcasted_iota(jnp.int32, (rows, rows), 1)
    pieces = pack_ref[5 * rows :, seqs * width : (seqs + 1) * width].astype(F32)[:3, :rows]
    other_gain = pieces[0:1] + pieces[1:2] + pieces[2:3]
    head_gain = jnp.concatenate(
        [jnp.sum(jnp.where(eye, h, 0.0), axis=1, keepdims=True) for h in (hg_ref[...], other_gain)], axis=0
    )
    scaled = turned_f32(o * norm * head_gain * gate).astype(BF16)
    out_copy.wait()
    columns = out_ref.shape[2]
    for b in range(blocks):
        at = slice(b * columns, (b + 1) * columns)
        w = jnp.concatenate([wo_ref[:, at], pack_ref[4 * rows : 5 * rows, at]], axis=0)
        out_ref[b] = mm(scaled, w).astype(BF16)


HBM = pl.BlockSpec(memory_space=pltpu.HBM)
ANY = pl.BlockSpec(memory_space=pl.ANY)
VMEM = pl.BlockSpec(memory_space=pltpu.VMEM)
SMEM = pl.BlockSpec(memory_space=pltpu.SMEM)


def local(
    tokens,
    norm_gain,
    w_query,
    w_key,
    w_value,
    w_gate,
    w_decay,
    w_beta,
    decay_rate,
    head_gain,
    w_out,
    state,
    prev_keys,
    prev_values,
    prev_decay,
    prev_beta,
    accepted,
):
    seqs, steps, lanes = tokens.shape
    half = seqs // 2
    n = half * steps
    rows, features = w_query.shape[1:]
    width = state.shape[-1]
    kv = lax.axis_size("kv")
    tp = lax.axis_index("tp")

    both = lax.all_gather(tokens.reshape(seqs * steps, lanes), "tp", axis=0)
    mine = lax.dynamic_slice_in_dim(both, tp * n, n, 1)
    copies = jnp.broadcast_to(mine[None], (kv, *mine.shape))
    gathered = lax.all_to_all(copies, "kv", split_axis=0, concat_axis=0, tiled=True)
    weights = [w.reshape(rows, features) for w in (w_query, w_key, w_value, w_gate)]
    w_own = w_out.reshape(rows, features)
    gain = head_gain.reshape(1, rows)
    commit = pl.pallas_call(
        commit_kernel,
        out_shape=(
            jax.ShapeDtypeStruct((seqs, rows, width), F32),
            jax.ShapeDtypeStruct((6 * rows, features), BF16),
        ),
        in_specs=[HBM] * 12,
        out_specs=(HBM, HBM),
        scratch_shapes=[
            pltpu.VMEM((seqs, rows, width), F32),
            pltpu.VMEM((seqs * steps, width), BF16),
            pltpu.VMEM((seqs * steps, rows), BF16),
            pltpu.VMEM((steps, seqs), F32),
            pltpu.VMEM((steps, seqs), F32),
            pltpu.VMEM((1, seqs), jnp.int32),
            pltpu.VMEM((1, rows), F32),
            pltpu.VMEM((5 * rows, features), BF16),
            pltpu.VMEM((seqs, rows, width), F32),
            pltpu.VMEM((rows, (half + 1) * width), BF16),
            pltpu.SemaphoreType.DMA((20,)),
        ],
        cost_estimate=pl.CostEstimate(flops=2 * 10**9, bytes_accessed=8 * 10**6, transcendentals=0),
        name="commit",
    )
    committed, pack = commit(
        state.reshape(seqs, rows, width),
        prev_keys.reshape(seqs * steps, width),
        prev_values.reshape(seqs * steps, rows),
        prev_decay[:, :, 0].T,
        prev_beta[:, :, 0].T,
        accepted.reshape(1, seqs),
        gain,
        *weights,
        w_own,
    )
    pack = lax.ppermute(pack, "tp", SWAP)
    columns = features // kv
    partial, committed = pl.pallas_call(
        layer_kernel,
        out_shape=(
            jax.ShapeDtypeStruct((kv, n, columns), BF16),
            jax.ShapeDtypeStruct((seqs, rows, width), F32),
        ),
        input_output_aliases={10: 1},
        in_specs=[VMEM] * 8 + [SMEM, VMEM, HBM, VMEM, HBM],
        out_specs=(VMEM, HBM),
        scratch_shapes=[
            pltpu.VMEM((half, rows, width), F32),
            pltpu.VMEM((6 * rows, features), BF16),
            pltpu.SemaphoreType.DMA((8,)),
        ],
        cost_estimate=pl.CostEstimate(flops=10**9, bytes_accessed=6 * 10**6, transcendentals=0),
        compiler_params=pltpu.CompilerParams(vmem_limit_bytes=48 * 2**20),
        name="layer",
    )(
        gathered,
        norm_gain.reshape(features // lanes, lanes),
        *weights,
        w_decay.T,
        w_beta.T,
        decay_rate,
        gain,
        committed,
        w_own,
        pack,
    )
    parts = lax.all_to_all(partial, "kv", split_axis=0, concat_axis=0, tiled=True)
    total = parts.astype(F32).sum(axis=0).astype(BF16)
    mixed = lax.dynamic_slice_in_dim(lax.all_gather(total, "tp", axis=0), tp * lanes, lanes, 2)
    return mixed.reshape(seqs, steps, lanes), committed.reshape(state.shape)


def solution(mesh):
    in_specs = (
        P(("grp", "dp"), None, ("kv", "tp")),
        P(),
        P("kv", "tp", None),
        P("kv", "tp", None),
        P("kv", "tp", None),
        P("kv", "tp", None),
        P(),
        P(),
        P("kv"),
        P("tp"),
        P("kv", "tp", None),
        P(("grp", "dp"), "kv", "tp", None),
        P(("grp", "dp"), None, "kv", None),
        P(("grp", "dp"), None, "kv", "tp"),
        P(("grp", "dp"), None, "kv"),
        P(("grp", "dp"), None, "kv"),
        P(("grp", "dp")),
    )
    out_specs = (P(("grp", "dp"), None, ("kv", "tp")), P(("grp", "dp"), "kv", "tp", None))
    return jax.shard_map(local, mesh=mesh, in_specs=in_specs, out_specs=out_specs, check_vma=False)
```

```python
import jax
import jax.numpy as jnp
from jax import lax
from jax.experimental import pallas as pl
from jax.experimental.pallas import tpu as pltpu
from jax.sharding import PartitionSpec as P


EPS = 1e-06
F32 = jnp.float32
BF16 = jnp.bfloat16
SWAP = [(0, 1), (1, 0)]


def mm(a, b, dims=((1,), (0,))):
    return lax.dot_general(
        a.astype(BF16), b.astype(BF16), (dims, ((), ())), preferred_element_type=F32
    )


NT = ((1,), (1,))


def high(a, b):
    return lax.dot_general(
        a, b, (((1,), (0,)), ((), ())), precision=lax.Precision.HIGHEST, preferred_element_type=F32
    )


def silu(x):
    return x / (1.0 + jnp.exp(-x))


def turned(x):
    n = x.shape[1]
    eye = lax.broadcasted_iota(jnp.int32, (n, n), 0) == lax.broadcasted_iota(jnp.int32, (n, n), 1)
    return mm(jnp.where(eye, 1.0, 0.0), x, NT)


def decays(d_row, steps):
    n = d_row.shape[1]
    shift = steps.bit_length() - 1
    i = lax.broadcasted_iota(jnp.int32, (n, n), 0)
    r = lax.broadcasted_iota(jnp.int32, (n, n), 1)
    same = (i >> shift) == (r >> shift)
    upto = same & (i <= r)
    before = same & (i < r)
    d_col = jnp.sum(jnp.where(i == r, d_row, 0.0), axis=1, keepdims=True)
    g_row = jnp.sum(jnp.where(upto, d_col, 0.0), axis=0, keepdims=True)
    g_col = jnp.sum(jnp.where(i == r, g_row, 0.0), axis=1, keepdims=True)
    between = jnp.where(upto, jnp.exp(jnp.where(upto, g_row - g_col, 0.0)), 0.0)
    last = jnp.sum(jnp.where(same & ((i & (steps - 1)) == steps - 1), g_col, 0.0), axis=0, keepdims=True)
    return g_row, g_col, last, between, before


def inverse(n):
    eye = lax.broadcasted_iota(jnp.int32, n.shape, 0) == lax.broadcasted_iota(jnp.int32, n.shape, 1)
    square = high(n, n)
    return jnp.where(eye, 1.0, 0.0) - n + square - high(n, square)


def own_products(states, keys_t, seqs, steps):
    product = mm(states, keys_t)
    rows, n = product.shape[0] // seqs, product.shape[1]
    shift = steps.bit_length() - 1
    seq_of = lax.broadcasted_iota(jnp.int32, (rows, n), 1) >> shift
    total = jnp.zeros((rows, n), F32)
    for s in range(seqs):
        total = total + jnp.where(seq_of == s, product[s * rows : (s + 1) * rows], 0.0)
    return total


def commit_kernel(
    state_hbm, keys_hbm, values_hbm, decay_hbm, beta_hbm, accepted_hbm, hg_hbm, wq_ref, wk_ref, wv_ref, wg_ref, wo_ref,
    out_ref, pack_ref, state_ref, keys_ref, values_ref, decay_ref, beta_ref, accepted_ref, hg_ref, weights, states, sent, sems,
):
    seqs, rows, width = state_ref.shape
    steps = decay_ref.shape[0]
    n = seqs * steps
    shift = steps.bit_length() - 1
    count = 5
    loads = [
        pltpu.make_async_copy(w, weights.at[k * rows : (k + 1) * rows], sems.at[k])
        for k, w in enumerate((wq_ref, wk_ref, wv_ref, wg_ref, wo_ref))
    ]
    small = [
        pltpu.make_async_copy(a, b, sems.at[count + 3 + k])
        for k, (a, b) in enumerate(
            (
                (keys_hbm, keys_ref),
                (decay_hbm, decay_ref),
                (beta_hbm, beta_ref),
                (accepted_hbm, accepted_ref),
                (values_hbm, values_ref),
                (hg_hbm, hg_ref),
                (state_hbm, state_ref),
            )
        )
    ]
    for load in small + loads:
        load.start()
    for load in small[:-1]:
        load.wait()
    keys = keys_ref[...].astype(F32)
    keys = keys * lax.rsqrt(jnp.sum(keys * keys, axis=-1, keepdims=True) + EPS)
    keys_t = turned_f32(keys)
    step_of = lax.broadcasted_iota(jnp.int32, (steps, n), 1) & (steps - 1)
    own_step = step_of == lax.broadcasted_iota(jnp.int32, (steps, n), 0)
    owner = lax.broadcasted_iota(jnp.int32, (seqs, n), 1) >> shift
    spread = jnp.where(owner == lax.broadcasted_iota(jnp.int32, (seqs, n), 0), 1.0, 0.0)
    taken = high(accepted_ref[...].astype(F32), spread)
    live = jnp.where(step_of[0:1].astype(F32) < taken - 0.5, 1.0, 0.0)
    d_row = -jnp.sum(jnp.where(own_step, high(decay_ref[...], spread), 0.0), axis=0, keepdims=True) * live
    b_row = jnp.sum(jnp.where(own_step, high(beta_ref[...], spread), 0.0), axis=0, keepdims=True) * live
    g_row, g_col, last, between, before = decays(d_row, steps)
    gram = mm(keys, keys, NT)
    nil = jnp.where(before, between * gram * b_row, 0.0)
    back = inverse(nil)
    values_t = turned(values_ref[...])
    small[-1].wait()
    state = state_ref[...]
    known = own_products(state.reshape(seqs * rows, width), keys_t, seqs, steps)
    stores = []
    for k, load in enumerate(loads):
        at = slice(k * rows, (k + 1) * rows)
        load.wait()
        stores.append(pltpu.make_async_copy(weights.at[at], pack_ref.at[at], sems.at[count + 10 + k]))
        stores[-1].start()
    u = high(b_row * (values_t - jnp.exp(g_row) * known), back) * jnp.exp(last - g_row)
    seq_of = lax.broadcasted_iota(jnp.int32, (rows, n), 1) >> shift
    spread_u = jnp.concatenate([jnp.where(seq_of == s, u, 0.0).astype(BF16) for s in range(seqs)], axis=0)
    update = mm(spread_u, keys)
    kept = jnp.broadcast_to(jnp.exp(g_col), (n, width))
    for s in range(seqs):
        at = s * steps + steps - 1
        states[s] = state[s] * kept[at : at + 1, :] + update[s * rows : (s + 1) * rows]
    half = seqs // 2
    tp = lax.axis_index("tp")
    for s in range(half):
        sent[:, s * width : (s + 1) * width] = states[(1 - tp) * half + s].astype(BF16)
    pieces, rest = [], jnp.concatenate([hg_ref[...], jnp.zeros((1, width - rows), F32)], axis=1)
    for _ in range(3):
        pieces.append(rest.astype(BF16).astype(F32))
        rest = rest - pieces[-1]
    pieces.append(jnp.zeros((rows - 3, width), F32))
    sent[:, half * width :] = jnp.concatenate(pieces, axis=0).astype(BF16)
    stores.append(pltpu.make_async_copy(states, out_ref, sems.at[count + 1]))
    stores[-1].start()
    columns = (half + 1) * width
    stores.append(pltpu.make_async_copy(sent, pack_ref.at[count * rows :, :columns], sems.at[count + 2]))
    stores[-1].start()
    for store in stores:
        store.wait()


def turned_f32(x):
    return turned(x.astype(BF16))


def layer_kernel(
    x_ref, gain_ref, wq_ref, wk_ref, wv_ref, wg_ref, decay_ref, beta_ref, rate_ref, hg_ref, committed_hbm, wo_ref, pack_hbm,
    out_ref, same_hbm, keep_ref, pack_ref, sems,
):
    blocks, _, n, lanes = x_ref.shape
    seqs, rows, width = keep_ref.shape
    steps = n // seqs
    heads = decay_ref.shape[0]
    tp = lax.axis_index("tp")
    head = lax.axis_index("kv")
    features = blocks * 2 * lanes
    copies = []

    def fetch(src, dst):
        copies.append(pltpu.make_async_copy(src, dst, sems.at[len(copies)]))
        copies[-1].start()
        return copies[-1]

    cuts = 4
    cut = features // cuts
    weight_copies = [
        fetch(pack_hbm.at[: 4 * rows, c * cut : (c + 1) * cut], pack_ref.at[: 4 * rows, c * cut : (c + 1) * cut])
        for c in range(cuts)
    ]
    columns = (seqs + 1) * width
    state_copies = [
        fetch(same_hbm.at[pl.ds(tp * seqs, seqs)], keep_ref),
        fetch(pack_hbm.at[5 * rows :, :columns], pack_ref.at[5 * rows :, :columns]),
    ]
    out_copy = fetch(pack_hbm.at[4 * rows : 5 * rows], pack_ref.at[4 * rows : 5 * rows])
    squares = jnp.zeros((n, lanes), F32)
    for b in range(blocks):
        for c in range(2):
            part = x_ref[b, c].astype(F32)
            squares = squares + part * part
    scale = lax.rsqrt(jnp.sum(squares, axis=-1, keepdims=True) / features + EPS)
    mine = jnp.zeros((4 * rows, n), F32)
    others = jnp.zeros((4 * rows, n), F32)
    gates = jnp.zeros((2 * heads, n), F32)
    for b in range(blocks):
        if b % (blocks // cuts) == 0:
            weight_copies[b // (blocks // cuts)].wait()
        at = slice(b * 2 * lanes, (b + 1) * 2 * lanes)
        pair = jnp.concatenate([x_ref[b, 0], x_ref[b, 1]], axis=1).astype(F32)
        gain = jnp.concatenate([gain_ref[2 * b : 2 * b + 1, :], gain_ref[2 * b + 1 : 2 * b + 2, :]], axis=1)
        normed = (pair * scale * gain).astype(BF16)
        w = jnp.concatenate([r[:, at] for r in (wq_ref, wk_ref, wv_ref, wg_ref)], axis=0)
        mine = mine + mm(w, normed, NT)
        others = others + mm(pack_ref[: 4 * rows, at], normed, NT)
        w = jnp.concatenate([decay_ref[:, at], beta_ref[:, at]], axis=0)
        gates = gates + mm(w, normed, NT)
    for copy in state_copies:
        copy.wait()
    mine = mine.astype(BF16).astype(F32)
    others = others.astype(BF16).astype(F32)

    def in_order(k):
        a, b = mine[k * rows : (k + 1) * rows], others[k * rows : (k + 1) * rows]
        return jnp.where(tp == 0, jnp.concatenate([a, b], axis=0), jnp.concatenate([b, a], axis=0))

    def own_first(k):
        return jnp.concatenate([mine[k * rows : (k + 1) * rows], others[k * rows : (k + 1) * rows]], axis=0)

    def unit(u):
        return u * lax.rsqrt(jnp.sum(u * u, axis=0, keepdims=True) + EPS)

    query = unit(silu(in_order(0))) * width ** (-0.5)
    key = unit(silu(in_order(1)))
    value = silu(own_first(2))
    gate = silu(own_first(3))
    at_head = lax.broadcasted_iota(jnp.int32, (heads, n), 0) == head
    decay_pre = jnp.sum(jnp.where(at_head, gates[:heads], 0.0), axis=0, keepdims=True)
    beta_pre = jnp.sum(jnp.where(at_head, gates[heads:], 0.0), axis=0, keepdims=True)
    softplus = jnp.maximum(decay_pre, 0.0) + jnp.log1p(jnp.exp(-jnp.abs(decay_pre)))
    d_row = -rate_ref[0] * softplus
    b_row = 1.0 / (1.0 + jnp.exp(-beta_pre))
    g_row, _, _, between, before = decays(d_row, steps)

    kept = keep_ref[...].reshape(seqs * rows, width).astype(BF16)
    got = jnp.concatenate([pack_ref[5 * rows :, s * width : (s + 1) * width] for s in range(seqs)], axis=0)

    def from_states(u):
        return jnp.concatenate([own_products(c, u, seqs, steps) for c in (kept, got)], axis=0)

    key_rows = turned_f32(key)
    nil = jnp.where(before, between * mm(key_rows, key) * b_row, 0.0)
    back = inverse(nil)
    u = high(b_row * (value - jnp.exp(g_row) * from_states(key)), back)
    o = jnp.exp(g_row) * from_states(query) + high(u, between * mm(key_rows, query))
    norm = lax.rsqrt(jnp.mean(o * o, axis=0, keepdims=True) + EPS)
    eye = lax.broadcasted_iota(jnp.int32, (rows, rows), 0) == lax.broadcasted_iota(jnp.int32, (rows, rows), 1)
    pieces = pack_ref[5 * rows :, seqs * width : (seqs + 1) * width].astype(F32)[:3, :rows]
    other_gain = pieces[0:1] + pieces[1:2] + pieces[2:3]
    head_gain = jnp.concatenate(
        [jnp.sum(jnp.where(eye, h, 0.0), axis=1, keepdims=True) for h in (hg_ref[...], other_gain)], axis=0
    )
    scaled = turned_f32(o * norm * head_gain * gate).astype(BF16)
    out_copy.wait()
    columns = out_ref.shape[2]
    for b in range(blocks):
        at = slice(b * columns, (b + 1) * columns)
        w = jnp.concatenate([wo_ref[:, at], pack_ref[4 * rows : 5 * rows, at]], axis=0)
        out_ref[b] = mm(scaled, w).astype(BF16)


HBM = pl.BlockSpec(memory_space=pltpu.HBM)
ANY = pl.BlockSpec(memory_space=pl.ANY)
VMEM = pl.BlockSpec(memory_space=pltpu.VMEM)
SMEM = pl.BlockSpec(memory_space=pltpu.SMEM)


def local(
    tokens,
    norm_gain,
    w_query,
    w_key,
    w_value,
    w_gate,
    w_decay,
    w_beta,
    decay_rate,
    head_gain,
    w_out,
    state,
    prev_keys,
    prev_values,
    prev_decay,
    prev_beta,
    accepted,
):
    seqs, steps, lanes = tokens.shape
    half = seqs // 2
    n = half * steps
    rows, features = w_query.shape[1:]
    width = state.shape[-1]
    kv = lax.axis_size("kv")
    tp = lax.axis_index("tp")

    first = tp == 0
    first, tokens = lax.optimization_barrier((first, tokens))
    both = lax.all_gather(tokens.reshape(seqs * steps, lanes), "tp", axis=0)
    mine = lax.dynamic_slice_in_dim(both, tp * n, n, 1)
    copies = jnp.broadcast_to(mine[None], (kv, *mine.shape))
    gathered = lax.all_to_all(copies, "kv", split_axis=0, concat_axis=0, tiled=True)
    weights = [w.reshape(rows, features) for w in (w_query, w_key, w_value, w_gate)]
    w_own = w_out.reshape(rows, features)
    gain = head_gain.reshape(1, rows)
    commit = pl.pallas_call(
        commit_kernel,
        out_shape=(
            jax.ShapeDtypeStruct((seqs, rows, width), F32),
            jax.ShapeDtypeStruct((6 * rows, features), BF16),
        ),
        in_specs=[HBM] * 12,
        out_specs=(HBM, HBM),
        scratch_shapes=[
            pltpu.VMEM((seqs, rows, width), F32),
            pltpu.VMEM((seqs * steps, width), BF16),
            pltpu.VMEM((seqs * steps, rows), BF16),
            pltpu.VMEM((steps, seqs), F32),
            pltpu.VMEM((steps, seqs), F32),
            pltpu.VMEM((1, seqs), jnp.int32),
            pltpu.VMEM((1, rows), F32),
            pltpu.VMEM((5 * rows, features), BF16),
            pltpu.VMEM((seqs, rows, width), F32),
            pltpu.VMEM((rows, (half + 1) * width), BF16),
            pltpu.SemaphoreType.DMA((20,)),
        ],
        cost_estimate=pl.CostEstimate(flops=2 * 10**9, bytes_accessed=8 * 10**6, transcendentals=0),
        name="commit",
    )
    committed, pack = commit(
        state.reshape(seqs, rows, width),
        prev_keys.reshape(seqs * steps, width),
        prev_values.reshape(seqs * steps, rows),
        prev_decay[:, :, 0].T,
        prev_beta[:, :, 0].T,
        accepted.reshape(1, seqs),
        gain,
        *weights,
        w_own,
    )
    pack = lax.ppermute(pack, "tp", SWAP)
    columns = features // kv
    partial, committed = pl.pallas_call(
        layer_kernel,
        out_shape=(
            jax.ShapeDtypeStruct((kv, n, columns), BF16),
            jax.ShapeDtypeStruct((seqs, rows, width), F32),
        ),
        input_output_aliases={10: 1},
        in_specs=[VMEM] * 8 + [SMEM, VMEM, HBM, VMEM, HBM],
        out_specs=(VMEM, HBM),
        scratch_shapes=[
            pltpu.VMEM((half, rows, width), F32),
            pltpu.VMEM((6 * rows, features), BF16),
            pltpu.SemaphoreType.DMA((8,)),
        ],
        cost_estimate=pl.CostEstimate(flops=10**9, bytes_accessed=6 * 10**6, transcendentals=0),
        compiler_params=pltpu.CompilerParams(vmem_limit_bytes=48 * 2**20),
        name="layer",
    )(
        gathered,
        norm_gain.reshape(features // lanes, lanes),
        *weights,
        w_decay.T,
        w_beta.T,
        decay_rate,
        gain,
        committed,
        w_own,
        pack,
    )
    parts = lax.all_to_all(partial, "kv", split_axis=0, concat_axis=0, tiled=True)
    total = parts.astype(F32).sum(axis=0).astype(BF16)
    joined = lax.all_gather(total, "tp", axis=0)
    mixed = jnp.where(first, joined[:, :, :lanes], joined[:, :, lanes:])
    return mixed.reshape(seqs, steps, lanes), committed.reshape(state.shape)


def solution(mesh):
    in_specs = (
        P(("grp", "dp"), None, ("kv", "tp")),
        P(),
        P("kv", "tp", None),
        P("kv", "tp", None),
        P("kv", "tp", None),
        P("kv", "tp", None),
        P(),
        P(),
        P("kv"),
        P("tp"),
        P("kv", "tp", None),
        P(("grp", "dp"), "kv", "tp", None),
        P(("grp", "dp"), None, "kv", None),
        P(("grp", "dp"), None, "kv", "tp"),
        P(("grp", "dp"), None, "kv"),
        P(("grp", "dp"), None, "kv"),
        P(("grp", "dp")),
    )
    out_specs = (P(("grp", "dp"), None, ("kv", "tp")), P(("grp", "dp"), "kv", "tp", None))
    return jax.shard_map(local, mesh=mesh, in_specs=in_specs, out_specs=out_specs, check_vma=False)
```

```python
import jax
import jax.numpy as jnp
from jax import lax
from jax.experimental import pallas as pl
from jax.experimental.pallas import tpu as pltpu
from jax.sharding import PartitionSpec as P

EPS = 1e-06
F32 = jnp.float32
BF16 = jnp.bfloat16
SWAP = [(0, 1), (1, 0)]


def mm(a, b, dims=((1,), (0,))):
    return lax.dot_general(
        a.astype(BF16), b.astype(BF16), (dims, ((), ())), preferred_element_type=F32
    )


NT = ((1,), (1,))


def high(a, b):
    return lax.dot_general(
        a, b, (((1,), (0,)), ((), ())), precision=lax.Precision.HIGHEST, preferred_element_type=F32
    )


def silu(x):
    return x / (1.0 + jnp.exp(-x))


def turned(x):
    n = x.shape[1]
    eye = lax.broadcasted_iota(jnp.int32, (n, n), 0) == lax.broadcasted_iota(jnp.int32, (n, n), 1)
    return mm(jnp.where(eye, 1.0, 0.0), x, NT)


def decays(d_row, steps):
    n = d_row.shape[1]
    shift = steps.bit_length() - 1
    i = lax.broadcasted_iota(jnp.int32, (n, n), 0)
    r = lax.broadcasted_iota(jnp.int32, (n, n), 1)
    same = (i >> shift) == (r >> shift)
    upto = same & (i <= r)
    before = same & (i < r)
    d_col = jnp.sum(jnp.where(i == r, d_row, 0.0), axis=1, keepdims=True)
    g_row = jnp.sum(jnp.where(upto, d_col, 0.0), axis=0, keepdims=True)
    g_col = jnp.sum(jnp.where(i == r, g_row, 0.0), axis=1, keepdims=True)
    between = jnp.where(upto, jnp.exp(jnp.where(upto, g_row - g_col, 0.0)), 0.0)
    last = jnp.sum(jnp.where(same & ((i & (steps - 1)) == steps - 1), g_col, 0.0), axis=0, keepdims=True)
    return g_row, g_col, last, between, before


def inverse(n):
    eye = lax.broadcasted_iota(jnp.int32, n.shape, 0) == lax.broadcasted_iota(jnp.int32, n.shape, 1)
    square = high(n, n)
    return jnp.where(eye, 1.0, 0.0) - n + square - high(n, square)


def own_products(states, keys_t, seqs, steps):
    product = mm(states, keys_t)
    rows, n = product.shape[0] // seqs, product.shape[1]
    shift = steps.bit_length() - 1
    seq_of = lax.broadcasted_iota(jnp.int32, (rows, n), 1) >> shift
    total = jnp.zeros((rows, n), F32)
    for s in range(seqs):
        total = total + jnp.where(seq_of == s, product[s * rows : (s + 1) * rows], 0.0)
    return total


def commit_kernel(
    state_hbm, keys_hbm, values_hbm, decay_hbm, beta_hbm, accepted_hbm, hg_hbm, wq_ref, wk_ref, wv_ref, wg_ref, wo_ref,
    out_ref, pack_ref, state_ref, keys_ref, values_ref, decay_ref, beta_ref, accepted_ref, hg_ref, weights, states, sent, sems,
):
    seqs, rows, width = state_ref.shape
    steps = decay_ref.shape[0]
    n = seqs * steps
    shift = steps.bit_length() - 1
    count = 5
    loads = [
        pltpu.make_async_copy(w, weights.at[k * rows : (k + 1) * rows], sems.at[k])
        for k, w in enumerate((wq_ref, wk_ref, wv_ref, wg_ref, wo_ref))
    ]
    small = [
        pltpu.make_async_copy(a, b, sems.at[count + 3 + k])
        for k, (a, b) in enumerate(
            (
                (keys_hbm, keys_ref),
                (decay_hbm, decay_ref),
                (beta_hbm, beta_ref),
                (accepted_hbm, accepted_ref),
                (values_hbm, values_ref),
                (hg_hbm, hg_ref),
                (state_hbm, state_ref),
            )
        )
    ]
    for load in small + loads:
        load.start()
    for load in small[:-1]:
        load.wait()
    keys = keys_ref[...].astype(F32)
    keys = keys * lax.rsqrt(jnp.sum(keys * keys, axis=-1, keepdims=True) + EPS)
    keys_t = turned_f32(keys)
    step_of = lax.broadcasted_iota(jnp.int32, (steps, n), 1) & (steps - 1)
    own_step = step_of == lax.broadcasted_iota(jnp.int32, (steps, n), 0)
    owner = lax.broadcasted_iota(jnp.int32, (seqs, n), 1) >> shift
    spread = jnp.where(owner == lax.broadcasted_iota(jnp.int32, (seqs, n), 0), 1.0, 0.0)
    taken = high(accepted_ref[...].astype(F32), spread)
    live = jnp.where(step_of[0:1].astype(F32) < taken - 0.5, 1.0, 0.0)
    d_row = -jnp.sum(jnp.where(own_step, high(decay_ref[...], spread), 0.0), axis=0, keepdims=True) * live
    b_row = jnp.sum(jnp.where(own_step, high(beta_ref[...], spread), 0.0), axis=0, keepdims=True) * live
    g_row, g_col, last, between, before = decays(d_row, steps)
    gram = mm(keys, keys, NT)
    nil = jnp.where(before, between * gram * b_row, 0.0)
    back = inverse(nil)
    values_t = turned(values_ref[...])
    small[-1].wait()
    state = state_ref[...]
    known = own_products(state.reshape(seqs * rows, width), keys_t, seqs, steps)
    stores = []
    for k, load in enumerate(loads):
        at = slice(k * rows, (k + 1) * rows)
        load.wait()
        stores.append(pltpu.make_async_copy(weights.at[at], pack_ref.at[at], sems.at[count + 10 + k]))
        stores[-1].start()
    u = high(b_row * (values_t - jnp.exp(g_row) * known), back) * jnp.exp(last - g_row)
    seq_of = lax.broadcasted_iota(jnp.int32, (rows, n), 1) >> shift
    spread_u = jnp.concatenate([jnp.where(seq_of == s, u, 0.0).astype(BF16) for s in range(seqs)], axis=0)
    update = mm(spread_u, keys)
    kept = jnp.broadcast_to(jnp.exp(g_col), (n, width))
    for s in range(seqs):
        at = s * steps + steps - 1
        states[s] = state[s] * kept[at : at + 1, :] + update[s * rows : (s + 1) * rows]
    half = seqs // 2
    tp = lax.axis_index("tp")
    for s in range(half):
        sent[:, s * width : (s + 1) * width] = states[(1 - tp) * half + s].astype(BF16)
    pieces, rest = [], jnp.concatenate([hg_ref[...], jnp.zeros((1, width - rows), F32)], axis=1)
    for _ in range(3):
        pieces.append(rest.astype(BF16).astype(F32))
        rest = rest - pieces[-1]
    pieces.append(jnp.zeros((rows - 3, width), F32))
    sent[:, half * width :] = jnp.concatenate(pieces, axis=0).astype(BF16)
    stores.append(pltpu.make_async_copy(states, out_ref, sems.at[count + 1]))
    stores[-1].start()
    columns = (half + 1) * width
    stores.append(pltpu.make_async_copy(sent, pack_ref.at[count * rows :, :columns], sems.at[count + 2]))
    stores[-1].start()
    for store in stores:
        store.wait()


def turned_f32(x):
    return turned(x.astype(BF16))


def layer_kernel(
    x_ref, gain_ref, wq_ref, wk_ref, wv_ref, wg_ref, decay_ref, beta_ref, rate_ref, hg_ref, committed_hbm, wo_ref, pack_hbm,
    out_ref, same_hbm, keep_ref, pack_ref, sems,
):
    blocks, _, n, lanes = x_ref.shape
    seqs, rows, width = keep_ref.shape
    steps = n // seqs
    heads = decay_ref.shape[0]
    tp = lax.axis_index("tp")
    head = lax.axis_index("kv")
    features = blocks * 2 * lanes
    copies = []

    def fetch(src, dst):
        copies.append(pltpu.make_async_copy(src, dst, sems.at[len(copies)]))
        copies[-1].start()
        return copies[-1]

    cuts = 4
    cut = features // cuts
    weight_copies = [
        fetch(pack_hbm.at[: 4 * rows, c * cut : (c + 1) * cut], pack_ref.at[: 4 * rows, c * cut : (c + 1) * cut])
        for c in range(cuts)
    ]
    columns = (seqs + 1) * width
    state_copies = [
        fetch(same_hbm.at[pl.ds(tp * seqs, seqs)], keep_ref),
        fetch(pack_hbm.at[5 * rows :, :columns], pack_ref.at[5 * rows :, :columns]),
    ]
    out_copy = fetch(pack_hbm.at[4 * rows : 5 * rows], pack_ref.at[4 * rows : 5 * rows])
    squares = jnp.zeros((n, lanes), F32)
    for b in range(blocks):
        for c in range(2):
            part = x_ref[b, c].astype(F32)
            squares = squares + part * part
    scale = lax.rsqrt(jnp.sum(squares, axis=-1, keepdims=True) / features + EPS)
    mine = jnp.zeros((4 * rows, n), F32)
    others = jnp.zeros((4 * rows, n), F32)
    gates = jnp.zeros((2 * heads, n), F32)
    for b in range(blocks):
        if b % (blocks // cuts) == 0:
            weight_copies[b // (blocks // cuts)].wait()
        at = slice(b * 2 * lanes, (b + 1) * 2 * lanes)
        pair = jnp.concatenate([x_ref[b, 0], x_ref[b, 1]], axis=1).astype(F32)
        gain = jnp.concatenate([gain_ref[2 * b : 2 * b + 1, :], gain_ref[2 * b + 1 : 2 * b + 2, :]], axis=1)
        normed = (pair * scale * gain).astype(BF16)
        w = jnp.concatenate([r[:, at] for r in (wq_ref, wk_ref, wv_ref, wg_ref)], axis=0)
        mine = mine + mm(w, normed, NT)
        others = others + mm(pack_ref[: 4 * rows, at], normed, NT)
        w = jnp.concatenate([decay_ref[:, at], beta_ref[:, at]], axis=0)
        gates = gates + mm(w, normed, NT)
    for copy in state_copies:
        copy.wait()
    mine = mine.astype(BF16).astype(F32)
    others = others.astype(BF16).astype(F32)

    def in_order(k):
        a, b = mine[k * rows : (k + 1) * rows], others[k * rows : (k + 1) * rows]
        return jnp.where(tp == 0, jnp.concatenate([a, b], axis=0), jnp.concatenate([b, a], axis=0))

    def own_first(k):
        return jnp.concatenate([mine[k * rows : (k + 1) * rows], others[k * rows : (k + 1) * rows]], axis=0)

    def unit(u):
        return u * lax.rsqrt(jnp.sum(u * u, axis=0, keepdims=True) + EPS)

    query = unit(silu(in_order(0))) * width ** (-0.5)
    key = unit(silu(in_order(1)))
    value = silu(own_first(2))
    gate = silu(own_first(3))
    at_head = lax.broadcasted_iota(jnp.int32, (heads, n), 0) == head
    decay_pre = jnp.sum(jnp.where(at_head, gates[:heads], 0.0), axis=0, keepdims=True)
    beta_pre = jnp.sum(jnp.where(at_head, gates[heads:], 0.0), axis=0, keepdims=True)
    softplus = jnp.maximum(decay_pre, 0.0) + jnp.log1p(jnp.exp(-jnp.abs(decay_pre)))
    d_row = -rate_ref[0] * softplus
    b_row = 1.0 / (1.0 + jnp.exp(-beta_pre))
    g_row, _, _, between, before = decays(d_row, steps)

    kept = keep_ref[...].reshape(seqs * rows, width).astype(BF16)
    got = jnp.concatenate([pack_ref[5 * rows :, s * width : (s + 1) * width] for s in range(seqs)], axis=0)

    def from_states(u):
        return jnp.concatenate([own_products(c, u, seqs, steps) for c in (kept, got)], axis=0)

    key_rows = turned_f32(key)
    nil = jnp.where(before, between * mm(key_rows, key) * b_row, 0.0)
    back = inverse(nil)
    u = high(b_row * (value - jnp.exp(g_row) * from_states(key)), back)
    o = jnp.exp(g_row) * from_states(query) + high(u, between * mm(key_rows, query))
    norm = lax.rsqrt(jnp.mean(o * o, axis=0, keepdims=True) + EPS)
    eye = lax.broadcasted_iota(jnp.int32, (rows, rows), 0) == lax.broadcasted_iota(jnp.int32, (rows, rows), 1)
    pieces = pack_ref[5 * rows :, seqs * width : (seqs + 1) * width].astype(F32)[:3, :rows]
    other_gain = pieces[0:1] + pieces[1:2] + pieces[2:3]
    head_gain = jnp.concatenate(
        [jnp.sum(jnp.where(eye, h, 0.0), axis=1, keepdims=True) for h in (hg_ref[...], other_gain)], axis=0
    )
    scaled = turned_f32(o * norm * head_gain * gate).astype(BF16)
    out_copy.wait()
    columns = out_ref.shape[2]
    for b in range(blocks):
        at = slice(b * columns, (b + 1) * columns)
        w = jnp.concatenate([wo_ref[:, at], pack_ref[4 * rows : 5 * rows, at]], axis=0)
        out_ref[b] = mm(scaled, w).astype(BF16)


HBM = pl.BlockSpec(memory_space=pltpu.HBM)
ANY = pl.BlockSpec(memory_space=pl.ANY)
VMEM = pl.BlockSpec(memory_space=pltpu.VMEM)
SMEM = pl.BlockSpec(memory_space=pltpu.SMEM)


def local(
    tokens,
    norm_gain,
    w_query,
    w_key,
    w_value,
    w_gate,
    w_decay,
    w_beta,
    decay_rate,
    head_gain,
    w_out,
    state,
    prev_keys,
    prev_values,
    prev_decay,
    prev_beta,
    accepted,
):
    seqs, steps, lanes = tokens.shape
    half = seqs // 2
    n = half * steps
    rows, features = w_query.shape[1:]
    width = state.shape[-1]
    kv = lax.axis_size("kv")
    tp = lax.axis_index("tp")

    first = tp == 0
    first, tokens = lax.optimization_barrier((first, tokens))
    both = lax.all_gather(tokens.reshape(seqs * steps, lanes), "tp", axis=0)
    mine = lax.dynamic_slice_in_dim(both, tp * n, n, 1)
    (both, state) = lax.optimization_barrier((both, state))
    weights = [w.reshape(rows, features) for w in (w_query, w_key, w_value, w_gate)]
    w_own = w_out.reshape(rows, features)
    gain = head_gain.reshape(1, rows)
    committed, pack = pl.pallas_call(
        commit_kernel,
        out_shape=(
            jax.ShapeDtypeStruct((seqs, rows, width), F32),
            jax.ShapeDtypeStruct((6 * rows, features), BF16),
        ),
        in_specs=[HBM] * 12,
        out_specs=(HBM, HBM),
        scratch_shapes=[
            pltpu.VMEM((seqs, rows, width), F32),
            pltpu.VMEM((seqs * steps, width), BF16),
            pltpu.VMEM((seqs * steps, rows), BF16),
            pltpu.VMEM((steps, seqs), F32),
            pltpu.VMEM((steps, seqs), F32),
            pltpu.VMEM((1, seqs), jnp.int32),
            pltpu.VMEM((1, rows), F32),
            pltpu.VMEM((5 * rows, features), BF16),
            pltpu.VMEM((seqs, rows, width), F32),
            pltpu.VMEM((rows, (half + 1) * width), BF16),
            pltpu.SemaphoreType.DMA((20,)),
        ],
        cost_estimate=pl.CostEstimate(flops=2 * 10**9, bytes_accessed=8 * 10**6, transcendentals=0),
        name="commit",
    )(
        state.reshape(seqs, rows, width),
        prev_keys.reshape(seqs * steps, width),
        prev_values.reshape(seqs * steps, rows),
        prev_decay[:, :, 0].T,
        prev_beta[:, :, 0].T,
        accepted.reshape(1, seqs),
        gain,
        *weights,
        w_own,
    )
    pack = lax.ppermute(pack, "tp", SWAP)
    gathered = lax.all_gather(mine, "kv", axis=0)
    columns = features // kv
    partial, committed = pl.pallas_call(
        layer_kernel,
        out_shape=(
            jax.ShapeDtypeStruct((kv, n, columns), BF16),
            jax.ShapeDtypeStruct((seqs, rows, width), F32),
        ),
        input_output_aliases={10: 1},
        in_specs=[VMEM] * 8 + [SMEM, VMEM, HBM, VMEM, HBM],
        out_specs=(VMEM, HBM),
        scratch_shapes=[
            pltpu.VMEM((half, rows, width), F32),
            pltpu.VMEM((6 * rows, features), BF16),
            pltpu.SemaphoreType.DMA((8,)),
        ],
        cost_estimate=pl.CostEstimate(flops=10**9, bytes_accessed=6 * 10**6, transcendentals=0),
        compiler_params=pltpu.CompilerParams(vmem_limit_bytes=48 * 2**20),
        name="layer",
    )(
        gathered,
        norm_gain.reshape(features // lanes, lanes),
        *weights,
        w_decay.T,
        w_beta.T,
        decay_rate,
        gain,
        committed,
        w_own,
        pack,
    )
    parts = lax.all_to_all(partial, "kv", split_axis=0, concat_axis=0, tiled=True)
    total = parts.astype(F32).sum(axis=0).astype(BF16)
    joined = lax.all_gather(total, "tp", axis=0)
    mixed = jnp.where(first, joined[:, :, :lanes], joined[:, :, lanes:])
    return mixed.reshape(seqs, steps, lanes), committed.reshape(state.shape)


def solution(mesh):
    in_specs = (
        P(("grp", "dp"), None, ("kv", "tp")),
        P(),
        P("kv", "tp", None),
        P("kv", "tp", None),
        P("kv", "tp", None),
        P("kv", "tp", None),
        P(),
        P(),
        P("kv"),
        P("tp"),
        P("kv", "tp", None),
        P(("grp", "dp"), "kv", "tp", None),
        P(("grp", "dp"), None, "kv", None),
        P(("grp", "dp"), None, "kv", "tp"),
        P(("grp", "dp"), None, "kv"),
        P(("grp", "dp"), None, "kv"),
        P(("grp", "dp")),
    )
    out_specs = (P(("grp", "dp"), None, ("kv", "tp")), P(("grp", "dp"), "kv", "tp", None))
    return jax.shard_map(local, mesh=mesh, in_specs=in_specs, out_specs=out_specs, check_vma=False)
```
